32 devices in a mesh: rep: 2 (over x), fs: 8 (over z, y), tp: 2 (over core).
Axes of the slice: x: 2, y: 2, z: 4, core: 2. Of those that a mesh axis runs over, the one named last changes fastest.
Arguments:
- tokens: bfloat16 [4096, 2048], P(('rep', 'fs', 'tp')), may hold values from -6 to 6
- mix_gain: float32 [2048], replicated, may hold values from 0.1 to 1.9
- conv_in_weight: bfloat16 [2048, 1024], P('fs', 'tp'), may hold values from -0.125 to 0.125
- gate_outer_weight: bfloat16 [2048, 1024], P('fs', 'tp'), may hold values from -0.125 to 0.125
- gate_inner_weight: bfloat16 [2048, 1024], P('fs', 'tp'), may hold values from -0.125 to 0.125
- conv_taps: float32 [3, 1024], P(None, 'tp'), may hold values from -3.5 to 3.5
- out_weight: bfloat16 [1024, 2048], P('tp', 'fs'), may hold values from -0.1875 to 0.1875
- ff_gain: float32 [2048], replicated, may hold values from 0.1 to 1.9
- up_weight: bfloat16 [2048, 8192], P('fs', 'tp'), may hold values from -0.125 to 0.125
- down_weight: bfloat16 [8192, 2048], P('tp', 'fs'), may hold values from -0.0625 to 0.0625
Outputs:
- layer_out: bfloat16 [4096, 2048], P(('rep', 'fs', 'tp'))
The draws below stay inside these ranges and needn't reach their ends.
All inputs are finite; a program needn't handle non-finite values.
Results may differ from the reference program's by a relative error of at most 0.023.
Values may be sent and summed in bfloat16 or wider, within the bound.
A program may use at most 128 MiB of HBM per device.

```python
import jax
import jax.numpy as jnp
from jax import lax

D = 2048
CONV = 1024
FF = 8192
TAPS = 3
SEQ = 256
TOKENS = 4096
CONV_DEV = 512
FF_DEV = 4096


def block_levels(own_key, extent, shards, least, largest):
    def one(dim, shards_of):
        draws = jax.random.uniform(jax.random.fold_in(jax.random.fold_in(own_key, 6), dim), (shards_of,), jnp.float32, least / len(shards), largest / len(shards))
        return jnp.repeat(jnp.exp(draws), extent[dim] // shards_of).reshape((-1,) + (1,) * (len(extent) - dim - 1))

    loudness = one(*shards[0])
    for cut in shards[1:]:
        loudness = loudness * one(*cut)
    return loudness


def noise(rng, extent, spread, bound, split=(), held_as=jnp.bfloat16):
    result = spread * jax.random.normal(rng, extent, jnp.float32)
    if split:
        result = result * block_levels(rng, extent, split, -0.22, 0.18)
    return jnp.clip(result, -bound, bound).astype(held_as)


def setup_inputs(seed: int = 0) -> dict:
    keys = jax.random.split(jax.random.key(seed), 11)
    tokens = noise(keys[0], (TOKENS, D), 1.0, 6.0, ((0, 32),))
    mix_gain = jnp.clip(1.0 + 0.18 * jax.random.normal(keys[1], (D,), jnp.float32), 0.1, 1.9)
    conv_in_weight = noise(keys[2], (D, CONV), D ** -0.5, 0.125, ((0, 8), (1, 2)))
    gate_outer_weight = noise(keys[3], (D, CONV), D ** -0.5, 0.125, ((0, 8), (1, 2)))
    gate_inner_weight = noise(keys[4], (D, CONV), D ** -0.5, 0.125, ((0, 8), (1, 2)))
    conv_taps = noise(keys[5], (TAPS, CONV), TAPS ** -0.5, 3.5, ((1, 2),), jnp.float32)
    out_weight = noise(keys[6], (CONV, D), CONV ** -0.5, 0.1875, ((0, 2), (1, 8)))
    ff_gain = jnp.clip(1.0 + 0.18 * jax.random.normal(keys[7], (D,), jnp.float32), 0.1, 1.9)
    up_weight = noise(keys[8], (D, FF), D ** -0.5, 0.125, ((0, 8), (1, 2)))
    down_weight = noise(keys[9], (FF, D), FF ** -0.5, 0.0625, ((0, 2), (1, 8)))
    return {"tokens": tokens, "mix_gain": mix_gain, "conv_in_weight": conv_in_weight, "gate_outer_weight": gate_outer_weight, "gate_inner_weight": gate_inner_weight, "conv_taps": conv_taps, "out_weight": out_weight, "ff_gain": ff_gain, "up_weight": up_weight, "down_weight": down_weight}


eps = 1e-06

def rms_scale(values, gain):
    widened = values.astype(jnp.float32)
    inverse = lax.rsqrt(lax.optimization_barrier(jnp.mean(widened * widened, axis=-1, keepdims=True)) + eps)
    return (widened * inverse * gain).astype(jnp.bfloat16)

def block_sum(activ, weight, width):
    blocks = activ.shape[1] // width

    def step(index, total):
        lefts = lax.dynamic_slice_in_dim(activ, index * width, width, 1)
        rights = lax.dynamic_slice_in_dim(weight, index * width, width, 0)
        rounded = jnp.dot(lefts, rights, preferred_element_type=jnp.float32).astype(jnp.bfloat16)
        rounded = lax.optimization_barrier(rounded)
        return total + rounded.astype(jnp.float32)
    initial = jnp.zeros((activ.shape[0], weight.shape[1]), jnp.float32)
    return lax.fori_loop(0, blocks, step, initial)

def reference(tokens, mix_gain, conv_in_weight, gate_outer_weight, gate_inner_weight, conv_taps, out_weight, ff_gain, up_weight, down_weight):
    normed = rms_scale(tokens, mix_gain)
    conv_input = jnp.dot(normed, conv_in_weight, preferred_element_type=jnp.float32).astype(jnp.bfloat16)
    gate_outer = jnp.dot(normed, gate_outer_weight, preferred_element_type=jnp.float32).astype(jnp.bfloat16)
    gate_inner = jnp.dot(normed, gate_inner_weight, preferred_element_type=jnp.float32).astype(jnp.bfloat16)
    gated = gate_inner.astype(jnp.float32) * conv_input.astype(jnp.float32)
    gated = gated.reshape(TOKENS // SEQ, SEQ, CONV)
    padded = jnp.pad(gated, ((0, 0), (TAPS - 1, 0), (0, 0)))
    convolved = conv_taps[0] * padded[:, 0:SEQ] + conv_taps[1] * padded[:, 1:SEQ + 1] + conv_taps[2] * padded[:, 2:SEQ + 2]
    convolved = convolved.reshape(TOKENS, CONV)
    mixed = (gate_outer.astype(jnp.float32) * convolved).astype(jnp.bfloat16)
    resid = (tokens.astype(jnp.float32) + block_sum(mixed, out_weight, CONV_DEV)).astype(jnp.bfloat16)
    normed_ff = rms_scale(resid, ff_gain)
    preact = jnp.dot(normed_ff, up_weight, preferred_element_type=jnp.float32)
    hidden = jnp.square(jax.nn.relu(preact)).astype(jnp.bfloat16)
    return (resid.astype(jnp.float32) + block_sum(hidden, down_weight, FF_DEV)).astype(jnp.bfloat16)
```

```python
import functools

import jax
import jax.numpy as jnp
from jax import lax
from jax.experimental import pallas as pl
from jax.experimental.pallas import tpu as pltpu
from jax.sharding import Mesh, PartitionSpec as P

eps = 1e-06


def rms_scale(values, gain):
    widened = values.astype(jnp.float32)
    inverse = lax.rsqrt(jnp.mean(widened * widened, axis=-1, keepdims=True) + eps)
    return (widened * inverse * gain).astype(jnp.bfloat16)


GROUP = ("rep", "near", "tp")


def gather_rows(block, near):
    rows, width = block.shape[0], block.shape[1] // near
    if near > 1:
        block = lax.all_to_all(
            block.reshape(rows, near, width).transpose(1, 0, 2), "near", 0, 0, tiled=True
        ).reshape(near * rows, width)
    return lax.all_gather(block, "far", axis=0, tiled=True)


def own_part(block, axis, rep):
    size = block.shape[axis] // rep
    return lax.dynamic_slice_in_dim(block, lax.axis_index("rep") * size, size, axis)


def on_device(rep, near, tp, tokens, mix_gain, conv_in, outer, inner, taps, out_w, ff_gain, up_w, down_w):
    seq_rows = tokens.shape[0] * tp
    depth = up_w.shape[0]
    parts = [own_part(w, 1, rep) for w in (conv_in, outer, inner)]
    width = parts[0].shape[1] // near
    trio = jnp.concatenate([p.reshape(depth, near, width) for p in parts], 2).reshape(depth, -1)
    trio = gather_rows(trio, near)
    out_part = own_part(out_w, 0, rep)
    out_part = out_part.reshape(near, width, -1).transpose(1, 0, 2).reshape(width, -1)
    out_full = gather_rows(out_part, near).reshape(-1, width, out_w.shape[1])
    up_full = gather_rows(own_part(up_w, 1, rep), near)
    down_part = own_part(down_w, 0, rep)
    hid = down_part.shape[0] // near
    down_part = down_part.reshape(near, hid, -1).transpose(1, 0, 2).reshape(hid, -1)
    down_full = gather_rows(down_part, near).reshape(-1, hid, down_w.shape[1])

    taps = own_part(taps, 1, rep)
    taps = lax.dynamic_slice_in_dim(taps, lax.axis_index("near") * width, width, 1)

    normed = lax.all_gather(rms_scale(tokens, mix_gain), GROUP, axis=0, tiled=True)
    proj = jnp.dot(normed, trio, preferred_element_type=jnp.float32).astype(jnp.bfloat16)
    proj = proj.astype(jnp.float32).reshape(-1, seq_rows, 3 * width)
    gated = proj[..., 2 * width :] * proj[..., :width]
    padded = jnp.pad(gated, ((0, 0), (2, 0), (0, 0)))
    convolved = sum(taps[k] * padded[:, k : seq_rows + k] for k in range(3))
    mixed = (proj[..., width : 2 * width] * convolved).astype(jnp.bfloat16)
    mixed = mixed.reshape(-1, width)

    def project(lefts, rights):
        whole = rights.transpose(1, 0, 2).reshape(lefts.shape[1], -1)
        partial = jnp.dot(lefts, whole, preferred_element_type=jnp.float32)
        return lax.psum_scatter(
            partial.astype(jnp.bfloat16), GROUP, scatter_dimension=0, tiled=True
        ).astype(jnp.float32)

    resid = (tokens.astype(jnp.float32) + project(mixed, out_full)).astype(jnp.bfloat16)
    normed_ff = lax.all_gather(rms_scale(resid, ff_gain), GROUP, axis=0, tiled=True)
    preact = jnp.dot(normed_ff, up_full, preferred_element_type=jnp.float32)
    hidden = jnp.square(jax.nn.relu(preact)).astype(jnp.bfloat16)
    return (resid.astype(jnp.float32) + project(hidden, down_full)).astype(jnp.bfloat16)


def layer_kernel(
    far,
    tok_ref, mix_gain_ref, conv_ref, outer_ref, inner_ref, taps_ref, outw_ref, ff_gain_ref, upw_ref, dnw_ref,
    o_ref,
    trio, outb, upb, dnb, stage, toks, toks_ff,
    part, sib, xs, xr, zs_, zr, part_ff, sib_ff, xs_ff, xr_ff, zs_ff, zr_ff,
    hidden, resid,
    local_sem, stage_sem, w_send, y_send, w_recv,
    ag_send, ag_recv, sib_send, sib_recv, x_send, x_recv, z_send, z_recv,
):
    r, z, y, t = (lax.axis_index(name) for name in ("rep", "far", "near", "tp"))
    rows = tok_ref.shape[0]
    seq = 2 * rows
    width = trio.shape[1] // 3
    depth, hid = upw_ref.shape[0], upb.shape[1]
    cols = dnw_ref.shape[1]
    group = 2 * cols
    bf16, f32 = jnp.bfloat16, jnp.float32

    pair, e = lax.div(z, 2), lax.rem(z, 2)
    edge = lax.rem(pair + e + 1, 2)
    zp = z + 1 - 2 * e
    zm = far - 1 - z
    zd = far - 1 - zp
    line = (z, zp, zm, zd)
    c = r * 2 + e
    cx, cz, cd = (1 - r) * 2 + e, r * 2 + 1 - e, (1 - r) * 2 + 1 - e
    q_own, q_other = r * 2 + edge, r * 2 + 1 - edge

    sibling = (r, z, y, 1 - t)
    beside = (r, z, 1 - y, t)
    across = (1 - r, z, y, t)
    partner = (r, zp, y, t)

    def al(v, n):
        return pl.multiple_of(v, n)

    def push(a, b, s, q, where):
        return pltpu.make_async_remote_copy(
            src_ref=a, dst_ref=b, send_sem=s, recv_sem=q, device_id=where, device_id_type=pl.DeviceIdType.MESH
        )

    def place(k, zs, ys):
        p = zs * 2 + ys
        if k == 0:
            return trio.at[pl.ds(al(p * depth, depth), depth), :]
        if k == 1:
            return outb.at[:, pl.ds(al(p * cols, cols), cols)]
        if k == 2:
            return upb.at[pl.ds(al(p * depth, depth), depth), :]
        return dnb.at[:, pl.ds(al(p * cols, cols), cols)]

    def share(k, q):
        if k == 1:
            return outw_ref.at[pl.ds(al(q * width, width), width), :]
        if k == 2:
            return upw_ref.at[:, pl.ds(al(q * hid, hid), hid)]
        return dnw_ref.at[pl.ds(al(q * hid, hid), hid), :]

    def trio_copies(dst, q, sems):
        return [
            pltpu.make_async_copy(
                w.at[:, pl.ds(al(q * width, width), width)],
                dst.at[:, pl.ds(j * width, width)],
                sems.at[j],
            )
            for j, w in enumerate((conv_ref, outer_ref, inner_ref))
        ]

    own_trio = trio_copies(place(0, z, y), q_own, local_sem)
    other_trio = trio_copies(stage, q_other, stage_sem)
    own_rest = [None] + [
        pltpu.make_async_copy(share(k, q_own), place(k, z, y), local_sem.at[2 + k]) for k in (1, 2, 3)
    ]

    def own_src(k):
        return place(0, z, y) if k == 0 else share(k, q_own)

    def other_src(k):
        return stage if k == 0 else share(k, q_other)

    def w_copy(k, i):
        a = own_src(k) if i == 1 else other_src(k)
        return push(
            a, place(k, z, y), w_send.at[k, i], w_recv.at[k, z * 2 + y], (r, (zp, zm, zd)[i], y, t)
        )

    def y_copy(k, j):
        at = place(k, line[j], y)
        a = own_src(k) if j == 0 else at
        return push(a, at, y_send.at[k, j], w_recv.at[k, line[j] * 2 + y], beside)

    def w_start(k):
        for i in range(3):
            w_copy(k, i).start()

    def landed(k, j, ys):
        at = place(k, line[j], ys)
        push(at, at, y_send.at[k, j], w_recv.at[k, line[j] * 2 + ys], beside).wait_recv()

    def arrive(k, j):
        landed(k, j, y)
        y_copy(k, j).start()

    def norm(values, gain_ref):
        inverse = lax.rsqrt(jnp.mean(values * values, axis=-1, keepdims=True) + eps)
        return (values * inverse * gain_ref[...]).astype(bf16)

    def slot(buf, s, core):
        return buf.at[pl.ds(al((s * 2 + core) * rows, rows), rows), :]

    def ag_copy(g, buf, i):
        s, core, where = (
            (c, t, partner), (c, t, across), (c, t, sibling),
            (cz, t, across), (cz, t, sibling), (cx, t, sibling), (cd, t, sibling),
        )[i]
        at = slot(buf, s, core)
        return push(at, at, ag_send.at[g, i], ag_recv.at[g, s * 2 + core], where)

    def ag_wait(g, buf, s, core):
        at = slot(buf, s, core)
        push(at, at, ag_send.at[g, 0], ag_recv.at[g, s * 2 + core], sibling).wait_recv()

    def ag_start(g, buf):
        for i in range(3):
            ag_copy(g, buf, i).start()

    def ag_relay(g, buf, s, sends):
        ag_wait(g, buf, s, t)
        for i in sends:
            ag_copy(g, buf, i).start()

    def sib_copy(n, s, buf, land, lo, size):
        at = buf.at[pl.ds(al(s * seq + (1 - t) * rows, rows), rows), pl.ds(lo, size)]
        to = land.at[pl.ds(al(s * rows, rows), rows), pl.ds(lo, size)]
        return push(at, to, sib_send.at[n, s], sib_recv.at[n, s], sibling)

    def x_copy(n, j, send, land, lo, size):
        return push(
            send.at[j, :, pl.ds(lo, size)], land.at[j, :, pl.ds(lo, size)], x_send.at[n, j], x_recv.at[n, j], across
        )

    def z_copy(n, send, land, lo, size):
        return push(send.at[:, pl.ds(lo, size)], land.at[:, pl.ds(lo, size)], z_send.at[n], z_recv.at[n], partner)

    def both(s, buf, land, lo, size):
        return (
            buf[pl.ds(al(s * seq + t * rows, rows), rows), pl.ds(lo, size)].astype(f32)
            + land[pl.ds(al(s * rows, rows), rows), pl.ds(lo, size)].astype(f32)
        )

    def reduce_x(n, buf, land, send, xland, lo, size):
        for j, s in ((0, cd), (1, cx)):
            send[j, :, pl.ds(lo, size)] = both(s, buf, land, lo, size).astype(bf16)
            x_copy(n, j, send, xland, lo, size).start()

    def reduce_z(n, buf, land, send, xland, zsend, zland, lo, size):
        x_copy(n, 0, send, xland, lo, size).wait_recv()
        total = both(cz, buf, land, lo, size) + xland[0, :, pl.ds(lo, size)].astype(f32)
        zsend[:, pl.ds(lo, size)] = total.astype(bf16)
        z_copy(n, zsend, zland, lo, size).start()

    def reduce_end(n, buf, land, send, xland, zsend, zland, lo, size):
        x_copy(n, 1, send, xland, lo, size).wait_recv()
        z_copy(n, zsend, zland, lo, size).wait_recv()
        return (
            both(c, buf, land, lo, size)
            + xland[1, :, pl.ds(lo, size)].astype(f32)
            + zland[:, pl.ds(lo, size)].astype(f32)
        )

    def seq_at(i):
        rr = lax.rem(r + 1 + lax.div(i, 2), 2)
        ee = lax.rem(e + 1 + lax.rem(i, 2), 2)
        return rr * 2 + ee

    for copy in own_trio + other_trio + own_rest[1:]:
        copy.start()
    slot(toks, c, t)[...] = norm(tok_ref[...].astype(f32), mix_gain_ref)
    ag_start(0, toks)
    for copy in own_trio + other_trio:
        copy.wait()
    for k in (0, 1):
        w_start(k)
        y_copy(k, 0).start()
    w_start(2)
    ag_relay(0, toks, cz, (3, 4))
    ag_relay(0, toks, cx, (5,))
    for k in (0, 1):
        arrive(k, 1)
    y_copy(2, 0).start()
    for j in (2, 3):
        for k in (0, 1):
            arrive(k, j)
    ag_relay(0, toks, cd, (6,))
    for s in (c, cx, cz, cd):
        ag_wait(0, toks, s, 1 - t)
    own_rest[1].wait()
    for j in range(4):
        for k in (0, 1):
            landed(k, j, 1 - y)

    mix_cols = outb.shape[1]
    taps = taps_ref[:, pl.ds(al(q_own * width, width), width)]

    @pl.loop(0, 4)
    def _(i):
        s = seq_at(i)
        x = toks[pl.ds(al(s * seq, seq), seq), :]
        proj = jnp.dot(x, trio[...], preferred_element_type=f32).astype(bf16).astype(f32)
        gated = proj[:, 2 * width :] * proj[:, :width]
        row = lax.broadcasted_iota(jnp.int32, gated.shape, 0)
        back1 = jnp.where(row < 1, 0.0, pltpu.roll(gated, 1, 0))
        back2 = jnp.where(row < 2, 0.0, pltpu.roll(gated, 2, 0))
        convolved = taps[0:1] * back2 + taps[1:2] * back1 + taps[2:3] * gated
        mixed = (proj[:, width : 2 * width] * convolved).astype(bf16)
        for lo in range(0, mix_cols, 1024):
            size = min(1024, mix_cols - lo)
            part[pl.ds(al(s * seq, seq), seq), pl.ds(lo, size)] = jnp.dot(
                mixed, outb[:, pl.ds(lo, size)], preferred_element_type=f32
            ).astype(bf16)
        sib_copy(0, s, part, sib, 0, mix_cols).start()

    mixer = (part, sib, xs, xr)
    for s in (cd, cx):
        sib_copy(0, s, part, sib, 0, mix_cols).wait_recv()
    for g in range(far):
        reduce_x(g, *mixer, g * group, group)
    for s in (cz, c):
        sib_copy(0, s, part, sib, 0, mix_cols).wait_recv()
    for g in range(far):
        reduce_z(g, *mixer, zs_, zr, g * group, group)
        if g == 2:
            arrive(2, 1)
    for g in range(far):
        at = pl.ds(g * group, group)
        total = reduce_end(g, *mixer, zs_, zr, g * group, group)
        resid[:, at] = (tok_ref[:, at].astype(f32) + total).astype(bf16)
    slot(toks_ff, c, t)[...] = norm(resid[...].astype(f32), ff_gain_ref)
    ag_start(1, toks_ff)
    w_start(3)
    for j in (2, 3):
        arrive(2, j)
    y_copy(3, 0).start()
    ag_relay(1, toks_ff, cz, (3, 4))
    ag_relay(1, toks_ff, cx, (5,))
    own_rest[2].wait()
    for j in range(4):
        landed(2, j, 1 - y)
    ag_relay(1, toks_ff, cd, (6,))
    for s in (c, cx, cz, cd):
        ag_wait(1, toks_ff, s, 1 - t)

    @pl.loop(0, 4)
    def _(s):
        x = toks_ff[pl.ds(al(s * seq, seq), seq), :]
        half = hid // 2
        for lo in (0, half):
            act = jnp.dot(x, upb[:, pl.ds(lo, half)], preferred_element_type=f32)
            hidden[pl.ds(al(s * seq, seq), seq), pl.ds(lo, half)] = jnp.square(jnp.maximum(act, 0.0)).astype(bf16)

    ff = (part_ff, sib_ff, xs_ff, xr_ff)

    def down(j):
        zs = line[j]
        lo = al(zs * group, group)

        @pl.loop(0, 4)
        def _(i):
            s = seq_at(i)
            part_ff[pl.ds(al(s * seq, seq), seq), pl.ds(lo, group)] = jnp.dot(
                hidden[pl.ds(al(s * seq, seq), seq), :], dnb[:, pl.ds(lo, group)], preferred_element_type=f32
            ).astype(bf16)
            sib_copy(1 + zs, s, part_ff, sib_ff, lo, group).start()

        for s in (cd, cx):
            sib_copy(1 + zs, s, part_ff, sib_ff, lo, group).wait_recv()
        reduce_x(far + zs, *ff, lo, group)
        for s in (cz, c):
            sib_copy(1 + zs, s, part_ff, sib_ff, lo, group).wait_recv()

    def finish(j):
        zs = line[j]
        lo = al(zs * group, group)
        reduce_z(far + zs, *ff, zs_ff, zr_ff, lo, group)

    own_rest[3].wait()
    landed(3, 0, 1 - y)
    down(0)
    for j in range(1, 4):
        arrive(3, j)
        finish(j - 1)
        landed(3, j, 1 - y)
        down(j)
    finish(3)
    for j in range(4):
        zs = line[j]
        lo = al(zs * group, group)
        total = reduce_end(far + zs, *ff, zs_ff, zr_ff, lo, group)
        o_ref[:, pl.ds(lo, group)] = (resid[:, pl.ds(lo, group)].astype(f32) + total).astype(bf16)

    for k in range(4):
        for i in range(3):
            w_copy(k, i).wait_send()
        for j in range(4):
            y_copy(k, j).wait_send()
    for g, buf in ((0, toks), (1, toks_ff)):
        for i in range(7):
            ag_copy(g, buf, i).wait_send()
    for s in range(4):
        sib_copy(0, s, part, sib, 0, mix_cols).wait_send()
        for n in range(far):
            sib_copy(1 + n, s, part_ff, sib_ff, n * group, group).wait_send()
    for n in range(far):
        lo = n * group
        for j in range(2):
            x_copy(n, j, xs, xr, lo, group).wait_send()
            x_copy(far + n, j, xs_ff, xr_ff, lo, group).wait_send()
        z_copy(n, zs_, zr, lo, group).wait_send()
        z_copy(far + n, zs_ff, zr_ff, lo, group).wait_send()


def fused_layer(far, tokens, mix_gain, conv_in, outer, inner, taps, out_w, ff_gain, up_w, down_w):
    bf16 = jnp.bfloat16
    rows, feat = tokens.shape
    depth, cols = up_w.shape[0], down_w.shape[1]
    width, hid = conv_in.shape[1] // 4, up_w.shape[1] // 4
    whole = 8 * rows
    vmem = pl.BlockSpec(memory_space=pltpu.VMEM)
    hbm = pl.BlockSpec(memory_space=pl.ANY)
    dma = pltpu.SemaphoreType.DMA
    block = [
        pltpu.VMEM((whole, feat), bf16),
        pltpu.VMEM((4 * rows, feat), bf16),
        pltpu.VMEM((2, rows, feat), bf16),
        pltpu.VMEM((2, rows, feat), bf16),
        pltpu.VMEM((rows, feat), bf16),
        pltpu.VMEM((rows, feat), bf16),
    ]
    return pl.pallas_call(
        functools.partial(layer_kernel, far),
        out_shape=jax.ShapeDtypeStruct((rows, feat), bf16),
        in_specs=[vmem, vmem, hbm, hbm, hbm, vmem, hbm, vmem, hbm, hbm],
        out_specs=vmem,
        scratch_shapes=[
            pltpu.VMEM((far * 2 * depth, 3 * width), bf16),
            pltpu.VMEM((width, far * 2 * cols), bf16),
            pltpu.VMEM((far * 2 * depth, hid), bf16),
            pltpu.VMEM((hid, far * 2 * cols), bf16),
            pltpu.VMEM((depth, 3 * width), bf16),
            pltpu.VMEM((whole, feat), bf16),
            pltpu.VMEM((whole, feat), bf16),
            *block,
            *block,
            pltpu.VMEM((whole, hid), bf16),
            pltpu.VMEM((rows, feat), bf16),
            dma((6,)),
            dma((3,)),
            dma((4, 3)),
            dma((4, 4)),
            dma((4, far * 2)),
            dma((2, 7)),
            dma((2, 8)),
            dma((1 + far, 4)),
            dma((1 + far, 4)),
            dma((2 * far, 2)),
            dma((2 * far, 2)),
            dma((2 * far,)),
            dma((2 * far,)),
        ],
        compiler_params=pltpu.CompilerParams(has_side_effects=True, vmem_limit_bytes=60 * 2**20),
    )(tokens, mix_gain[None], conv_in, outer, inner, taps, out_w, ff_gain[None], up_w, down_w)


def solution(mesh):
    rep, fs, tp = (mesh.shape[name] for name in ("rep", "fs", "tp"))
    near = 2 if fs % 2 == 0 else 1
    mesh4 = Mesh(mesh.devices.reshape(rep, fs // near, near, tp), ("rep", "far", "near", "tp"))
    fs_axes = ("far", "near")
    rows = P(("rep", "far", "near", "tp"), None)
    in_specs = (
        rows,
        P(),
        P(fs_axes, "tp"),
        P(fs_axes, "tp"),
        P(fs_axes, "tp"),
        P(None, "tp"),
        P("tp", fs_axes),
        P(),
        P(fs_axes, "tp"),
        P("tp", fs_axes),
    )

    def body(*args):
        if rep == 2 and near == 2 and tp == 2 and fs == 8:
            return fused_layer(fs // near, *args)
        return on_device(rep, near, tp, *args)

    return jax.shard_map(body, mesh=mesh4, in_specs=in_specs, out_specs=rows, check_vma=False)
```

```python
import functools

import jax
import jax.numpy as jnp
from jax import lax
from jax.experimental import pallas as pl
from jax.experimental.pallas import tpu as pltpu
from jax.sharding import Mesh, PartitionSpec as P

eps = 1e-06


def rms_scale(values, gain):
    widened = values.astype(jnp.float32)
    inverse = lax.rsqrt(jnp.mean(widened * widened, axis=-1, keepdims=True) + eps)
    return (widened * inverse * gain).astype(jnp.bfloat16)


GROUP = ("rep", "near", "tp")


def gather_rows(block, near):
    rows, width = block.shape[0], block.shape[1] // near
    if near > 1:
        block = lax.all_to_all(
            block.reshape(rows, near, width).transpose(1, 0, 2), "near", 0, 0, tiled=True
        ).reshape(near * rows, width)
    return lax.all_gather(block, "far", axis=0, tiled=True)


def own_part(block, axis, rep):
    size = block.shape[axis] // rep
    return lax.dynamic_slice_in_dim(block, lax.axis_index("rep") * size, size, axis)


def on_device(rep, near, tp, tokens, mix_gain, conv_in, outer, inner, taps, out_w, ff_gain, up_w, down_w):
    seq_rows = tokens.shape[0] * tp
    depth = up_w.shape[0]
    parts = [own_part(w, 1, rep) for w in (conv_in, outer, inner)]
    width = parts[0].shape[1] // near
    trio = jnp.concatenate([p.reshape(depth, near, width) for p in parts], 2).reshape(depth, -1)
    trio = gather_rows(trio, near)
    out_part = own_part(out_w, 0, rep)
    out_part = out_part.reshape(near, width, -1).transpose(1, 0, 2).reshape(width, -1)
    out_full = gather_rows(out_part, near).reshape(-1, width, out_w.shape[1])
    up_full = gather_rows(own_part(up_w, 1, rep), near)
    down_part = own_part(down_w, 0, rep)
    hid = down_part.shape[0] // near
    down_part = down_part.reshape(near, hid, -1).transpose(1, 0, 2).reshape(hid, -1)
    down_full = gather_rows(down_part, near).reshape(-1, hid, down_w.shape[1])

    taps = own_part(taps, 1, rep)
    taps = lax.dynamic_slice_in_dim(taps, lax.axis_index("near") * width, width, 1)

    normed = lax.all_gather(rms_scale(tokens, mix_gain), GROUP, axis=0, tiled=True)
    proj = jnp.dot(normed, trio, preferred_element_type=jnp.float32).astype(jnp.bfloat16)
    proj = proj.astype(jnp.float32).reshape(-1, seq_rows, 3 * width)
    gated = proj[..., 2 * width :] * proj[..., :width]
    padded = jnp.pad(gated, ((0, 0), (2, 0), (0, 0)))
    convolved = sum(taps[k] * padded[:, k : seq_rows + k] for k in range(3))
    mixed = (proj[..., width : 2 * width] * convolved).astype(jnp.bfloat16)
    mixed = mixed.reshape(-1, width)

    def project(lefts, rights):
        whole = rights.transpose(1, 0, 2).reshape(lefts.shape[1], -1)
        partial = jnp.dot(lefts, whole, preferred_element_type=jnp.float32)
        return lax.psum_scatter(
            partial.astype(jnp.bfloat16), GROUP, scatter_dimension=0, tiled=True
        ).astype(jnp.float32)

    resid = (tokens.astype(jnp.float32) + project(mixed, out_full)).astype(jnp.bfloat16)
    normed_ff = lax.all_gather(rms_scale(resid, ff_gain), GROUP, axis=0, tiled=True)
    preact = jnp.dot(normed_ff, up_full, preferred_element_type=jnp.float32)
    hidden = jnp.square(jax.nn.relu(preact)).astype(jnp.bfloat16)
    return (resid.astype(jnp.float32) + project(hidden, down_full)).astype(jnp.bfloat16)


def visit_order(far):
    return [sorted(range(far), key=lambda s: (abs(s - z), s)) for z in range(far)]


def layer_kernel(
    far,
    tok_ref, mix_gain_ref, conv_ref, outer_ref, inner_ref, taps_ref, outw_ref, ff_gain_ref, upw_ref, dnw_ref,
    o_ref,
    trio, outb, upb, dnb, stage, toks, toks_ff,
    part, sib, xs, xr, ps, pr, part_ff, sib_ff, xs_ff, xr_ff, ps_ff, pr_ff,
    hidden, resid,
    local_sem, stage_sem, near_send, right_send, left_send, w_send, y_send, w_recv,
    ag_send, ag_recv, sib_send, sib_recv, x_send, x_recv, p_send, p_recv,
):
    r, z, y, t = (lax.axis_index(name) for name in ("rep", "far", "near", "tp"))
    rows = tok_ref.shape[0]
    seq = 2 * rows
    width = trio.shape[1] // 3
    depth, hid = upw_ref.shape[0], upb.shape[1]
    cols = dnw_ref.shape[1]
    group, strip = 2 * cols, cols // 2
    bf16, f32 = jnp.bfloat16, jnp.float32

    pair, half_z = lax.div(z, 2), lax.rem(z, 2)
    edge = lax.rem(pair + half_z + 1, 2)
    zp = z + 1 - 2 * half_z
    zm = far - 1 - z
    zd = far - 1 - zp
    line = (z, zp, zm, zd)
    side = (y, half_z)
    own, cross, pal, diag = (
        [rr * 2 + ee for ee in ends]
        for rr, ends in ((r, side), (1 - r, side), (r, (1 - y, 1 - half_z)), (1 - r, (1 - y, 1 - half_z)))
    )
    q_own, q_other = r * 2 + edge, r * 2 + 1 - edge

    sibling = (r, z, y, 1 - t)
    beside = (r, z, 1 - y, t)
    across = (1 - r, z, y, t)
    partner = (beside, (r, zp, y, t))

    def al(v, n):
        return pl.multiple_of(v, n)

    def push(a, b, s, q, where):
        return pltpu.make_async_remote_copy(
            src_ref=a, dst_ref=b, send_sem=s, recv_sem=q, device_id=where, device_id_type=pl.DeviceIdType.MESH
        )

    def place(k, zs, ys):
        p = zs * 2 + ys
        if k == 0:
            return trio.at[pl.ds(al(p * depth, depth), depth), :]
        if k == 1:
            return outb.at[:, pl.ds(al(p * cols, cols), cols)]
        if k == 2:
            return upb.at[pl.ds(al(p * depth, depth), depth), :]
        lo = ((zs * 2 + k - 3) * 2 + ys) * strip
        return dnb.at[:, pl.ds(al(lo, strip), strip)]

    def share(k, q):
        if k == 1:
            return outw_ref.at[pl.ds(al(q * width, width), width), :]
        if k == 2:
            return upw_ref.at[:, pl.ds(al(q * hid, hid), hid)]
        return dnw_ref.at[pl.ds(al(q * hid, hid), hid), pl.ds((k - 3) * strip, strip)]

    def trio_copies(dst, q, sems):
        return [
            pltpu.make_async_copy(
                w.at[:, pl.ds(al(q * width, width), width)],
                dst.at[:, pl.ds(j * width, width)],
                sems.at[j],
            )
            for j, w in enumerate((conv_ref, outer_ref, inner_ref))
        ]

    own_trio = trio_copies(place(0, z, y), r * 2 + y, local_sem)
    other_trio = trio_copies(stage, r * 2 + 1 - y, stage_sem)
    own_rest = [None] + [
        pltpu.make_async_copy(share(k, r * 2 + y if k == 1 else q_own), place(k, z, y), local_sem.at[2 + k])
        for k in (1, 2, 3, 4)
    ]

    def near_copy(k):
        a = stage if k == 0 else share(k, r * 2 + 1 - y)
        return push(a, place(k, z, y), near_send.at[k], w_recv.at[k, z * 2 + y], beside)

    def hop(k, zs, ys, step, sems):
        p = zs * 2 + ys
        at = place(k, zs, ys)
        return push(at, at, sems.at[k, p], w_recv.at[k, p], (r, z + step, y, t))

    order = visit_order(far)

    def nth(j):
        zs = jnp.int32(order[0][j])
        for c in range(1, far):
            zs = jnp.where(z == c, order[c][j], zs)
        return zs

    def send_on(k, zs, ys):
        @pl.when(jnp.logical_and(zs <= z, z + 1 < far))
        def _():
            hop(k, zs, ys, 1, right_send).start()

        @pl.when(jnp.logical_and(zs >= z, z > 0))
        def _():
            hop(k, zs, ys, -1, left_send).start()

    def mix_landed(k, zs, ys):
        at = place(k, zs, ys)
        push(at, at, near_send.at[k], w_recv.at[k, zs * 2 + ys], beside).wait_recv()
        send_on(k, zs, ys)

    def w_copy(k, i):
        a = share(k, q_own if i == 1 else q_other)
        return push(
            a, place(k, z, y), w_send.at[k - 2, i], w_recv.at[k, z * 2 + y], (r, (zp, zm, zd)[i], y, t)
        )

    def w_when(k, i, at_edge):
        @pl.when(edge == at_edge)
        def _():
            w_copy(k, i).start()

    def y_copy(k, j):
        at = place(k, line[j], y)
        a = share(k, q_own) if j == 0 else at
        return push(a, at, y_send.at[k - 2, j], w_recv.at[k, line[j] * 2 + y], beside)

    def landed(k, j, ys):
        at = place(k, line[j], ys)
        push(at, at, y_send.at[k - 2, j], w_recv.at[k, line[j] * 2 + ys], beside).wait_recv()

    def arrive(k, j):
        landed(k, j, y)
        y_copy(k, j).start()

    def norm(values, gain_ref):
        inverse = lax.rsqrt(jnp.mean(values * values, axis=-1, keepdims=True) + eps)
        return (values * inverse * gain_ref[...]).astype(bf16)

    def slot(buf, s, core):
        return buf.at[pl.ds(al((s * 2 + core) * rows, rows), rows), :]

    def ag_copy(g, buf, i):
        s, core, where = (
            (own[g], t, partner[g]), (own[g], t, across), (own[g], t, sibling),
            (pal[g], t, across), (pal[g], t, sibling), (cross[g], t, sibling), (diag[g], t, sibling),
        )[i]
        at = slot(buf, s, core)
        return push(at, at, ag_send.at[g, i], ag_recv.at[g, s * 2 + core], where)

    def ag_wait(g, buf, s, core):
        at = slot(buf, s, core)
        push(at, at, ag_send.at[g, 0], ag_recv.at[g, s * 2 + core], sibling).wait_recv()

    def ag_start(g, buf):
        for i in range(3):
            ag_copy(g, buf, i).start()

    def ag_relay(g, buf, s, sends):
        ag_wait(g, buf, s, t)
        for i in sends:
            ag_copy(g, buf, i).start()

    def sib_copy(n, s, buf, land, lo, size):
        at = buf.at[pl.ds(al(s * seq + (1 - t) * rows, rows), rows), pl.ds(lo, size)]
        to = land.at[pl.ds(al(s * rows, rows), rows), pl.ds(lo, size)]
        return push(at, to, sib_send.at[n, s], sib_recv.at[n, s], sibling)

    def x_copy(n, j, send, land, lo, size):
        return push(
            send.at[j, :, pl.ds(lo, size)], land.at[j, :, pl.ds(lo, size)], x_send.at[n, j], x_recv.at[n, j], across
        )

    def p_copy(g, n, send, land, lo, size):
        return push(send.at[:, pl.ds(lo, size)], land.at[:, pl.ds(lo, size)], p_send.at[n], p_recv.at[n], partner[g])

    def both(s, buf, land, lo, size):
        return (
            buf[pl.ds(al(s * seq + t * rows, rows), rows), pl.ds(lo, size)].astype(f32)
            + land[pl.ds(al(s * rows, rows), rows), pl.ds(lo, size)].astype(f32)
        )

    mixer = (part, sib, xs, xr, ps, pr)
    ff = (part_ff, sib_ff, xs_ff, xr_ff, ps_ff, pr_ff)

    def reduce_x(g, n, lo, size):
        buf, land, send, xland, _, _ = (mixer, ff)[g]
        for j, s in ((0, diag[g]), (1, cross[g])):
            send[j, :, pl.ds(lo, size)] = both(s, buf, land, lo, size).astype(bf16)
            x_copy(n, j, send, xland, lo, size).start()

    def reduce_p(g, n, lo, size):
        buf, land, send, xland, psend, pland = (mixer, ff)[g]
        x_copy(n, 0, send, xland, lo, size).wait_recv()
        total = both(pal[g], buf, land, lo, size) + xland[0, :, pl.ds(lo, size)].astype(f32)
        psend[:, pl.ds(lo, size)] = total.astype(bf16)
        p_copy(g, n, psend, pland, lo, size).start()

    def reduce_end(g, n, lo, size):
        buf, land, send, xland, psend, pland = (mixer, ff)[g]
        x_copy(n, 1, send, xland, lo, size).wait_recv()
        p_copy(g, n, psend, pland, lo, size).wait_recv()
        return (
            both(own[g], buf, land, lo, size)
            + xland[1, :, pl.ds(lo, size)].astype(f32)
            + pland[:, pl.ds(lo, size)].astype(f32)
        )

    def seq_at(g, i):
        rr = lax.rem(r + 1 + lax.div(i, 2), 2)
        ee = lax.rem(side[g] + 1 + lax.rem(i, 2), 2)
        return rr * 2 + ee

    barrier = pltpu.get_barrier_semaphore()
    peers = (sibling, beside, across, partner[1], (r, zm, y, t), (r, zd, y, t))
    for where in peers:
        pl.semaphore_signal(barrier, inc=1, device_id=where, device_id_type=pl.DeviceIdType.MESH)
    for copy in other_trio + own_trio + own_rest[1:]:
        copy.start()
    slot(toks, own[0], t)[...] = norm(tok_ref[...].astype(f32), mix_gain_ref)
    pl.semaphore_wait(barrier, len(peers))
    for copy in other_trio:
        copy.wait()
    near_copy(0).start()
    near_copy(1).start()
    for copy in own_trio:
        copy.wait()
    send_on(0, z, y)
    own_rest[1].wait()
    send_on(1, z, y)
    ag_start(0, toks)
    for k in (0, 1):
        mix_landed(k, z, 1 - y)
    w_when(2, 0, 1)
    for k in (0, 1):
        for ys in (y, 1 - y):
            mix_landed(k, nth(1), ys)
    for k in (0, 1):
        for ys in (y, 1 - y):
            mix_landed(k, nth(2), ys)
    ag_relay(0, toks, pal[0], (3, 4))
    ag_relay(0, toks, cross[0], (5,))
    y_copy(2, 0).start()
    for k in (0, 1):
        for ys in (y, 1 - y):
            mix_landed(k, nth(3), ys)
    for k in (3, 4):
        y_copy(k, 0).start()
    w_when(2, 1, 0)
    w_when(2, 2, 1)
    ag_relay(0, toks, diag[0], (6,))
    for s in (own[0], cross[0], pal[0], diag[0]):
        ag_wait(0, toks, s, 1 - t)

    w_when(2, 0, 0)

    @pl.when(edge == 0)
    def _():
        arrive(2, 1)

    mix_cols = outb.shape[1]
    taps = taps_ref[:, pl.ds(al((r * 2 + y) * width, width), width)]

    @pl.loop(0, 4)
    def _(i):
        s = seq_at(0, i)
        x = toks[pl.ds(al(s * seq, seq), seq), :]
        proj = jnp.dot(x, trio[...], preferred_element_type=f32).astype(bf16).astype(f32)
        gated = proj[:, 2 * width :] * proj[:, :width]
        row = lax.broadcasted_iota(jnp.int32, gated.shape, 0)
        back1 = jnp.where(row < 1, 0.0, pltpu.roll(gated, 1, 0))
        back2 = jnp.where(row < 2, 0.0, pltpu.roll(gated, 2, 0))
        convolved = taps[0:1] * back2 + taps[1:2] * back1 + taps[2:3] * gated
        mixed = (proj[:, width : 2 * width] * convolved).astype(bf16)
        for lo in range(0, mix_cols, 1024):
            size = min(1024, mix_cols - lo)
            part[pl.ds(al(s * seq, seq), seq), pl.ds(lo, size)] = jnp.dot(
                mixed, outb[:, pl.ds(lo, size)], preferred_element_type=f32
            ).astype(bf16)
        sib_copy(0, s, part, sib, 0, mix_cols).start()

    for s in (diag[0], cross[0]):
        sib_copy(0, s, part, sib, 0, mix_cols).wait_recv()
    for n in range(far):
        reduce_x(0, n, n * group, group)
    for s in (pal[0], own[0]):
        sib_copy(0, s, part, sib, 0, mix_cols).wait_recv()
    for n in range(far):
        reduce_p(0, n, n * group, group)
        if n == 0:
            w_when(2, 1, 1)
            w_when(2, 2, 0)
        if n == 2:
            for k in (3, 4):
                w_when(k, 0, 1)
                w_when(k, 2, 1)

    @pl.when(edge == 1)
    def _():
        arrive(2, 1)

    for n in range(far):
        at = pl.ds(n * group, group)
        total = reduce_end(0, n, n * group, group)
        resid[:, at] = (tok_ref[:, at].astype(f32) + total).astype(bf16)
    slot(toks_ff, own[1], t)[...] = norm(resid[...].astype(f32), ff_gain_ref)
    ag_start(1, toks_ff)
    for j in (2, 3):
        arrive(2, j)
    for k in (3, 4):
        w_when(k, 1, 0)
        w_when(k, 0, 0)
    ag_relay(1, toks_ff, pal[1], (3, 4))
    ag_relay(1, toks_ff, cross[1], (5,))
    arrive(3, 1)
    w_when(3, 1, 1)
    w_when(3, 2, 0)
    own_rest[2].wait()
    for j in range(4):
        landed(2, j, 1 - y)

    def up(i):
        s = seq_at(1, 3 - i)
        ag_wait(1, toks_ff, s, 1 - t)
        x = toks_ff[pl.ds(al(s * seq, seq), seq), :]
        half = hid // 2
        for lo in (0, half):
            act = jnp.dot(x, upb[:, pl.ds(lo, half)], preferred_element_type=f32)
            hidden[pl.ds(al(s * seq, seq), seq), pl.ds(lo, half)] = jnp.square(jnp.maximum(act, 0.0)).astype(bf16)

    pl.loop(0, 3)(up)
    ag_relay(1, toks_ff, diag[1], (6,))
    arrive(4, 1)
    w_when(4, 1, 1)
    w_when(4, 2, 0)
    up(3)

    def down(j, h):
        m = line[j] * 2 + h
        lo = al(m * cols, cols)

        @pl.loop(0, 4)
        def _(i):
            s = seq_at(1, i)
            part_ff[pl.ds(al(s * seq, seq), seq), pl.ds(lo, cols)] = jnp.dot(
                hidden[pl.ds(al(s * seq, seq), seq), :], dnb[:, pl.ds(lo, cols)], preferred_element_type=f32
            ).astype(bf16)
            sib_copy(1 + m, s, part_ff, sib_ff, lo, cols).start()

        for s in (diag[1], cross[1]):
            sib_copy(1 + m, s, part_ff, sib_ff, lo, cols).wait_recv()
        reduce_x(1, far + m, lo, cols)
        for s in (pal[1], own[1]):
            sib_copy(1 + m, s, part_ff, sib_ff, lo, cols).wait_recv()

    def finish(j, h):
        m = line[j] * 2 + h
        reduce_p(1, far + m, al(m * cols, cols), cols)

    def end(j, h):
        m = line[j] * 2 + h
        total = reduce_end(1, far + m, al(m * cols, cols), cols)
        for ys in range(2):
            at = pl.ds(al(line[j] * group + ys * cols + h * strip, strip), strip)
            o_ref[:, at] = (resid[:, at].astype(f32) + total[:, ys * strip : (ys + 1) * strip]).astype(bf16)

    own_rest[3].wait()
    own_rest[4].wait()
    steps = [(0, 0), (0, 1), (1, 0), (1, 1), (2, 0), (3, 0), (2, 1), (3, 1)]
    ahead = {0: ((3, 2), (3, 3)), 2: ((4, 2),), 3: ((4, 3),)}
    for n, (j, h) in enumerate(steps):
        landed(3 + h, j, 1 - y)
        down(j, h)
        for block in ahead.get(n, ()):
            arrive(*block)
        if n > 0:
            finish(*steps[n - 1])
        if n > 2:
            end(*steps[n - 3])
    finish(*steps[-1])
    for step in steps[-3:]:
        end(*step)

    for k in (0, 1):
        near_copy(k).wait_send()
        for zs in range(far):
            for ys in range(2):
                @pl.when(jnp.logical_and(zs <= z, z + 1 < far))
                def _():
                    hop(k, zs, ys, 1, right_send).wait_send()

                @pl.when(jnp.logical_and(zs >= z, z > 0))
                def _():
                    hop(k, zs, ys, -1, left_send).wait_send()
    for k in (2, 3, 4):
        for i in range(3):
            w_copy(k, i).wait_send()
        for j in range(4):
            y_copy(k, j).wait_send()
    for g, buf in ((0, toks), (1, toks_ff)):
        for i in range(7):
            ag_copy(g, buf, i).wait_send()
    for s in range(4):
        sib_copy(0, s, part, sib, 0, mix_cols).wait_send()
    for n in range(far):
        lo = n * group
        for j in range(2):
            x_copy(n, j, xs, xr, lo, group).wait_send()
        p_copy(0, n, ps, pr, lo, group).wait_send()
    for m in range(2 * far):
        lo = m * cols
        for s in range(4):
            sib_copy(1 + m, s, part_ff, sib_ff, lo, cols).wait_send()
        for j in range(2):
            x_copy(far + m, j, xs_ff, xr_ff, lo, cols).wait_send()
        p_copy(1, far + m, ps_ff, pr_ff, lo, cols).wait_send()


def fused_layer(far, tokens, mix_gain, conv_in, outer, inner, taps, out_w, ff_gain, up_w, down_w):
    bf16 = jnp.bfloat16
    rows, feat = tokens.shape
    depth, cols = up_w.shape[0], down_w.shape[1]
    width, hid = conv_in.shape[1] // 4, up_w.shape[1] // 4
    whole = 8 * rows
    vmem = pl.BlockSpec(memory_space=pltpu.VMEM)
    hbm = pl.BlockSpec(memory_space=pl.ANY)
    dma = pltpu.SemaphoreType.DMA
    block = [
        pltpu.VMEM((whole, feat), bf16),
        pltpu.VMEM((4 * rows, feat), bf16),
        pltpu.VMEM((2, rows, feat), bf16),
        pltpu.VMEM((2, rows, feat), bf16),
        pltpu.VMEM((rows, feat), bf16),
        pltpu.VMEM((rows, feat), bf16),
    ]
    return pl.pallas_call(
        functools.partial(layer_kernel, far),
        out_shape=jax.ShapeDtypeStruct((rows, feat), bf16),
        in_specs=[vmem, vmem, hbm, hbm, hbm, vmem, hbm, vmem, hbm, hbm],
        out_specs=vmem,
        scratch_shapes=[
            pltpu.VMEM((far * 2 * depth, 3 * width), bf16),
            pltpu.VMEM((width, far * 2 * cols), bf16),
            pltpu.VMEM((far * 2 * depth, hid), bf16),
            pltpu.VMEM((hid, far * 2 * cols), bf16),
            pltpu.VMEM((depth, 3 * width), bf16),
            pltpu.VMEM((whole, feat), bf16),
            pltpu.VMEM((whole, feat), bf16),
            *block,
            *block,
            pltpu.VMEM((whole, hid), bf16),
            pltpu.VMEM((rows, feat), bf16),
            dma((7,)),
            dma((3,)),
            dma((2,)),
            dma((2, far * 2)),
            dma((2, far * 2)),
            dma((3, 3)),
            dma((3, 4)),
            dma((5, far * 2)),
            dma((2, 7)),
            dma((2, 8)),
            dma((1 + 2 * far, 4)),
            dma((1 + 2 * far, 4)),
            dma((3 * far, 2)),
            dma((3 * far, 2)),
            dma((3 * far,)),
            dma((3 * far,)),
        ],
        compiler_params=pltpu.CompilerParams(
            collective_id=0, has_side_effects=True, vmem_limit_bytes=60 * 2**20),
    )(tokens, mix_gain[None], conv_in, outer, inner, taps, out_w, ff_gain[None], up_w, down_w)


def solution(mesh):
    rep, fs, tp = (mesh.shape[name] for name in ("rep", "fs", "tp"))
    near = 2 if fs % 2 == 0 else 1
    mesh4 = Mesh(mesh.devices.reshape(rep, fs // near, near, tp), ("rep", "far", "near", "tp"))
    fs_axes = ("far", "near")
    rows = P(("rep", "far", "near", "tp"), None)
    in_specs = (
        rows,
        P(),
        P(fs_axes, "tp"),
        P(fs_axes, "tp"),
        P(fs_axes, "tp"),
        P(None, "tp"),
        P("tp", fs_axes),
        P(),
        P(fs_axes, "tp"),
        P("tp", fs_axes),
    )

    def body(*args):
        if rep == 2 and near == 2 and tp == 2 and fs == 8:
            return fused_layer(fs // near, *args)
        return on_device(rep, near, tp, *args)

    return jax.shard_map(body, mesh=mesh4, in_specs=in_specs, out_specs=rows, check_vma=False)
```

```python
import functools

import jax
import jax.numpy as jnp
from jax import lax
from jax.experimental import pallas as pl
from jax.experimental.pallas import tpu as pltpu
from jax.sharding import Mesh, PartitionSpec as P

eps = 1e-06


def rms_scale(values, gain):
    widened = values.astype(jnp.float32)
    inverse = lax.rsqrt(jnp.mean(widened * widened, axis=-1, keepdims=True) + eps)
    return (widened * inverse * gain).astype(jnp.bfloat16)


GROUP = ("rep", "near", "tp")


def gather_rows(block, near):
    rows, width = block.shape[0], block.shape[1] // near
    if near > 1:
        block = lax.all_to_all(
            block.reshape(rows, near, width).transpose(1, 0, 2), "near", 0, 0, tiled=True
        ).reshape(near * rows, width)
    return lax.all_gather(block, "far", axis=0, tiled=True)


def own_part(block, axis, rep):
    size = block.shape[axis] // rep
    return lax.dynamic_slice_in_dim(block, lax.axis_index("rep") * size, size, axis)


def on_device(rep, near, tp, tokens, mix_gain, conv_in, outer, inner, taps, out_w, ff_gain, up_w, down_w):
    seq_rows = tokens.shape[0] * tp
    depth = up_w.shape[0]
    parts = [own_part(w, 1, rep) for w in (conv_in, outer, inner)]
    width = parts[0].shape[1] // near
    trio = jnp.concatenate([p.reshape(depth, near, width) for p in parts], 2).reshape(depth, -1)
    trio = gather_rows(trio, near)
    out_part = own_part(out_w, 0, rep)
    out_part = out_part.reshape(near, width, -1).transpose(1, 0, 2).reshape(width, -1)
    out_full = gather_rows(out_part, near).reshape(-1, width, out_w.shape[1])
    up_full = gather_rows(own_part(up_w, 1, rep), near)
    down_part = own_part(down_w, 0, rep)
    hid = down_part.shape[0] // near
    down_part = down_part.reshape(near, hid, -1).transpose(1, 0, 2).reshape(hid, -1)
    down_full = gather_rows(down_part, near).reshape(-1, hid, down_w.shape[1])

    taps = own_part(taps, 1, rep)
    taps = lax.dynamic_slice_in_dim(taps, lax.axis_index("near") * width, width, 1)

    normed = lax.all_gather(rms_scale(tokens, mix_gain), GROUP, axis=0, tiled=True)
    proj = jnp.dot(normed, trio, preferred_element_type=jnp.float32).astype(jnp.bfloat16)
    proj = proj.astype(jnp.float32).reshape(-1, seq_rows, 3 * width)
    gated = proj[..., 2 * width :] * proj[..., :width]
    padded = jnp.pad(gated, ((0, 0), (2, 0), (0, 0)))
    convolved = sum(taps[k] * padded[:, k : seq_rows + k] for k in range(3))
    mixed = (proj[..., width : 2 * width] * convolved).astype(jnp.bfloat16)
    mixed = mixed.reshape(-1, width)

    def project(lefts, rights):
        whole = rights.transpose(1, 0, 2).reshape(lefts.shape[1], -1)
        partial = jnp.dot(lefts, whole, preferred_element_type=jnp.float32)
        return lax.psum_scatter(
            partial.astype(jnp.bfloat16), GROUP, scatter_dimension=0, tiled=True
        ).astype(jnp.float32)

    resid = (tokens.astype(jnp.float32) + project(mixed, out_full)).astype(jnp.bfloat16)
    normed_ff = lax.all_gather(rms_scale(resid, ff_gain), GROUP, axis=0, tiled=True)
    preact = jnp.dot(normed_ff, up_full, preferred_element_type=jnp.float32)
    hidden = jnp.square(jax.nn.relu(preact)).astype(jnp.bfloat16)
    return (resid.astype(jnp.float32) + project(hidden, down_full)).astype(jnp.bfloat16)


SEND, OWN, TAKE = range(3)
LATE = 6
PLAN = (
    {
        2: ((OWN, 2, 0), (OWN, 3, 0), (OWN, 4, 0), (OWN, 5, 0),),
        4: ((SEND, 2, 1), (SEND, 2, 0),),
        5: ((TAKE, 2, 1),),
        7: ((SEND, 2, 2),),
        12: ((TAKE, 2, 2), (TAKE, 2, 3), (SEND, 3, 0), (SEND, 3, 1),),
        13: ((SEND, 3, 2),),
        14: ((TAKE, 3, 1), (SEND, 4, 0), (SEND, 5, 0), (SEND, 4, 1), (SEND, 5, 1), (SEND, 4, 2), (SEND, 5, 2),),
        19: ((TAKE, 4, 1), (TAKE, 5, 1),),
        20: ((TAKE, 3, 2), (TAKE, 3, 3),),
        22: ((TAKE, 4, 2), (TAKE, 5, 2),),
        23: ((TAKE, 4, 3), (TAKE, 5, 3),),
    },
    {
        1: ((SEND, 2, 0),),
        2: ((SEND, 2, 2), (OWN, 2, 0), (OWN, 3, 0), (OWN, 4, 0), (OWN, 5, 0),),
        3: ((SEND, 3, 0), (SEND, 4, 0), (SEND, 5, 0),),
        6: ((TAKE, 2, 1), (SEND, 2, 1),),
        12: ((TAKE, 2, 2), (TAKE, 2, 3), (SEND, 3, 2),),
        13: ((SEND, 3, 1),),
        14: ((TAKE, 3, 1), (SEND, 4, 1), (SEND, 5, 1), (SEND, 4, 2), (SEND, 5, 2),),
        19: ((TAKE, 4, 1), (TAKE, 5, 1),),
        20: ((TAKE, 3, 2), (TAKE, 3, 3),),
        22: ((TAKE, 4, 2), (TAKE, 5, 2),),
        23: ((TAKE, 4, 3), (TAKE, 5, 3),),
    },
)


def visit_order(far):
    return [sorted(range(far), key=lambda s: (abs(s - z), s)) for z in range(far)]


def chip_kernel(
    far, edge,
    tok_ref, mix_gain_ref, conv_ref, outer_ref, inner_ref, taps_ref, outw_ref, ff_gain_ref, upw_ref, dnw_ref,
    o_ref,
    trio, outb, upb, dnb, stage, toks, toks_ff,
    part, sib, xs, xr, ps, pr, part_ff, sib_ff, xs_ff, xr_ff, ps_ff, pr_ff,
    hidden, resid, result, out_sem,
    local_sem, stage_sem, near_send, right_send, left_send, w_send, y_send, w_recv,
    ag_send, ag_recv, sib_send, sib_recv, x_send, x_recv, p_send, p_recv,
):
    r, z, y, t = (lax.axis_index(name) for name in ("rep", "far", "near", "tp"))
    rows = tok_ref.shape[0]
    seq = 2 * rows
    width = trio.shape[1] // 3
    depth = upw_ref.shape[0]
    unit = upw_ref.shape[1] // 32
    sizes = (8 * unit, 8 * unit)
    hid = sizes[edge]
    cols = dnw_ref.shape[1]
    group, strip = 2 * cols, cols // 2
    bf16, f32 = jnp.bfloat16, jnp.float32

    half_z = lax.rem(z, 2)
    zp = z + 1 - 2 * half_z
    zm = far - 1 - z
    zd = far - 1 - zp
    line = (z, zp, zm, zd)
    side = (y, half_z)
    own, cross, pal, diag = (
        [rr * 2 + ee for ee in ends]
        for rr, ends in ((r, side), (1 - r, side), (r, (1 - y, 1 - half_z)), (1 - r, (1 - y, 1 - half_z)))
    )

    def split(kind):
        return pl.ds(al(r * 16 * unit + kind * sizes[0], unit), sizes[kind])

    sibling = (r, z, y, 1 - t)
    beside = (r, z, 1 - y, t)
    across = (1 - r, z, y, t)
    partner = (beside, (r, zp, y, t))

    def al(v, n):
        return pl.multiple_of(v, n)

    def push(a, b, s, q, where):
        return pltpu.make_async_remote_copy(
            src_ref=a, dst_ref=b, send_sem=s, recv_sem=q, device_id=where, device_id_type=pl.DeviceIdType.MESH
        )

    def lines(k, size):
        half = size // 2
        return ((0, size), (0, half), (half, size - half))[k - 3]

    def place(k, zs, ys, kind=None):
        p = zs * 2 + ys
        if k == 0:
            return trio.at[pl.ds(al(p * depth, depth), depth), :]
        if k == 1:
            return outb.at[:, pl.ds(al(p * cols, cols), cols)]
        size = sizes[edge if kind is None else kind]
        if k == 2:
            return upb.at[pl.ds(al(p * depth, depth), depth), pl.ds(0, size)]
        lo = ((zs * 2 + min(k - 3, 1)) * 2 + ys) * strip
        top, some = lines(k, size)
        return dnb.at[pl.ds(top, some), pl.ds(al(lo, strip), strip)]

    def share(k, q):
        if k == 1:
            return outw_ref.at[pl.ds(al(q * width, width), width), :]
        if k == 2:
            return upw_ref.at[:, split(q)]
        top, some = lines(k, sizes[q])
        start = al(r * 16 * unit + q * sizes[0] + top, unit)
        return dnw_ref.at[pl.ds(start, some), pl.ds(min(k - 3, 1) * strip, strip)]

    def trio_copies(dst, q, sems):
        return [
            pltpu.make_async_copy(
                w.at[:, pl.ds(al(q * width, width), width)],
                dst.at[:, pl.ds(j * width, width)],
                sems.at[j],
            )
            for j, w in enumerate((conv_ref, outer_ref, inner_ref))
        ]

    own_trio = trio_copies(place(0, z, y), r * 2 + y, local_sem)
    other_trio = trio_copies(stage, r * 2 + 1 - y, stage_sem)
    own_rest = [None] + [
        pltpu.make_async_copy(share(k, r * 2 + y if k == 1 else edge), place(k, z, y), local_sem.at[2 + k])
        for k in (1, 2, 3, 4, 5)
    ]

    def near_copy(k):
        a = stage if k == 0 else share(k, r * 2 + 1 - y)
        return push(a, place(k, z, y), near_send.at[k], w_recv.at[k, z * 2 + y], beside)

    def hop(k, zs, ys, step, sems):
        p = zs * 2 + ys
        at = place(k, zs, ys)
        return push(at, at, sems.at[k, p], w_recv.at[k, p], (r, z + step, y, t))

    order = visit_order(far)

    def nth(j):
        zs = jnp.int32(order[0][j])
        for c in range(1, far):
            zs = jnp.where(z == c, order[c][j], zs)
        return zs

    def send_on(k, zs, ys):
        @pl.when(jnp.logical_and(zs <= z, z + 1 < far))
        def _():
            hop(k, zs, ys, 1, right_send).start()

        @pl.when(jnp.logical_and(zs >= z, z > 0))
        def _():
            hop(k, zs, ys, -1, left_send).start()

    def mix_landed(k, zs, ys):
        at = place(k, zs, ys)
        push(at, at, near_send.at[k], w_recv.at[k, zs * 2 + ys], beside).wait_recv()
        send_on(k, zs, ys)

    def w_copy(k, i):
        kind = edge if i == 1 else 1 - edge
        return push(
            share(k, kind), place(k, z, y, kind), w_send.at[k - 2, i], w_recv.at[k, z * 2 + y], (r, (zp, zm, zd)[i], y, t)
        )

    def y_copy(k, j):
        at = place(k, line[j], y)
        a = share(k, edge) if j == 0 else at
        return push(a, at, y_send.at[k - 2, j], w_recv.at[k, line[j] * 2 + y], beside)

    def landed(k, j, ys):
        at = place(k, line[j], ys)
        push(at, at, y_send.at[k - 2, j], w_recv.at[k, line[j] * 2 + ys], beside).wait_recv()

    def arrive(k, j):
        landed(k, j, y)
        y_copy(k, j).start()

    def at(point):
        for what, k, i in PLAN[edge].get(point, ()):
            if what == SEND:
                w_copy(k, i).start()
            elif what == OWN:
                y_copy(k, 0).start()
            else:
                arrive(k, i)

    def norm(values, gain_ref):
        inverse = lax.rsqrt(jnp.mean(values * values, axis=-1, keepdims=True) + eps)
        return (values * inverse * gain_ref[...]).astype(bf16)

    def slot(buf, s, core):
        return buf.at[pl.ds(al((s * 2 + core) * rows, rows), rows), :]

    def ag_copy(g, buf, i):
        s, core, where = (
            (own[g], t, partner[g]), (own[g], t, across), (own[g], t, sibling),
            (pal[g], t, across), (pal[g], t, sibling), (cross[g], t, sibling), (diag[g], t, sibling),
        )[i]
        at = slot(buf, s, core)
        return push(at, at, ag_send.at[g, i], ag_recv.at[g, s * 2 + core], where)

    def ag_wait(g, buf, s, core):
        at = slot(buf, s, core)
        push(at, at, ag_send.at[g, 0], ag_recv.at[g, s * 2 + core], sibling).wait_recv()

    def ag_start(g, buf):
        for i in range(3):
            ag_copy(g, buf, i).start()

    def ag_relay(g, buf, s, sends):
        ag_wait(g, buf, s, t)
        for i in sends:
            ag_copy(g, buf, i).start()

    def sib_copy(n, s, buf, land, lo, size):
        at = buf.at[pl.ds(al(s * seq + (1 - t) * rows, rows), rows), pl.ds(lo, size)]
        to = land.at[pl.ds(al(s * rows, rows), rows), pl.ds(lo, size)]
        return push(at, to, sib_send.at[n, s], sib_recv.at[n, s], sibling)

    def x_copy(n, j, send, land, lo, size):
        return push(
            send.at[j, :, pl.ds(lo, size)], land.at[j, :, pl.ds(lo, size)], x_send.at[n, j], x_recv.at[n, j], across
        )

    def p_copy(g, n, send, land, lo, size):
        return push(send.at[:, pl.ds(lo, size)], land.at[:, pl.ds(lo, size)], p_send.at[n], p_recv.at[n], partner[g])

    def both(s, buf, land, lo, size):
        return (
            buf[pl.ds(al(s * seq + t * rows, rows), rows), pl.ds(lo, size)].astype(f32)
            + land[pl.ds(al(s * rows, rows), rows), pl.ds(lo, size)].astype(f32)
        )

    mixer = (part, sib, xs, xr, ps, pr)
    ff = (part_ff, sib_ff, xs_ff, xr_ff, ps_ff, pr_ff)

    def reduce_x(g, n, lo, size):
        buf, land, send, xland, _, _ = (mixer, ff)[g]
        for j, s in ((0, diag[g]), (1, cross[g])):
            send[j, :, pl.ds(lo, size)] = both(s, buf, land, lo, size).astype(bf16)
            x_copy(n, j, send, xland, lo, size).start()

    def reduce_p(g, n, lo, size):
        buf, land, send, xland, psend, pland = (mixer, ff)[g]
        x_copy(n, 0, send, xland, lo, size).wait_recv()
        total = both(pal[g], buf, land, lo, size) + xland[0, :, pl.ds(lo, size)].astype(f32)
        psend[:, pl.ds(lo, size)] = total.astype(bf16)
        p_copy(g, n, psend, pland, lo, size).start()

    def reduce_end(g, n, lo, size):
        buf, land, send, xland, psend, pland = (mixer, ff)[g]
        x_copy(n, 1, send, xland, lo, size).wait_recv()
        p_copy(g, n, psend, pland, lo, size).wait_recv()
        return (
            both(own[g], buf, land, lo, size)
            + xland[1, :, pl.ds(lo, size)].astype(f32)
            + pland[:, pl.ds(lo, size)].astype(f32)
        )

    def seq_at(g, i):
        rr = lax.rem(r + 1 + lax.div(i, 2), 2)
        ee = lax.rem(side[g] + 1 + lax.rem(i, 2), 2)
        return rr * 2 + ee

    barrier = pltpu.get_barrier_semaphore()
    peers = (sibling, beside, across, partner[1], (r, zm, y, t), (r, zd, y, t))
    for where in peers:
        pl.semaphore_signal(barrier, inc=1, device_id=where, device_id_type=pl.DeviceIdType.MESH)
    for copy in other_trio + own_trio + own_rest[1:]:
        copy.start()
    slot(toks, own[0], t)[...] = norm(tok_ref[...].astype(f32), mix_gain_ref)
    pl.semaphore_wait(barrier, len(peers))
    for copy in other_trio:
        copy.wait()
    near_copy(0).start()
    near_copy(1).start()
    for copy in own_trio:
        copy.wait()
    send_on(0, z, y)
    own_rest[1].wait()
    send_on(1, z, y)
    ag_start(0, toks)
    at(0)
    for k in (0, 1):
        mix_landed(k, z, 1 - y)
    at(1)
    for k in (0, 1):
        for ys in (y, 1 - y):
            mix_landed(k, nth(1), ys)
    at(2)
    for k in (0, 1):
        for ys in (y, 1 - y):
            mix_landed(k, nth(2), ys)
    at(3)
    ag_relay(0, toks, pal[0], (3, 4))
    ag_relay(0, toks, cross[0], (5,))
    for k in (0, 1):
        for ys in (y, 1 - y):
            mix_landed(k, nth(3), ys)
    at(4)
    ag_relay(0, toks, diag[0], (6,))
    for s in (own[0], cross[0], pal[0], diag[0]):
        ag_wait(0, toks, s, 1 - t)
    at(5)

    mix_cols = outb.shape[1]
    taps = taps_ref[:, pl.ds(al((r * 2 + y) * width, width), width)]

    @pl.loop(0, 4)
    def _(i):
        s = seq_at(0, i)
        x = toks[pl.ds(al(s * seq, seq), seq), :]
        proj = jnp.dot(x, trio[...], preferred_element_type=f32).astype(bf16).astype(f32)
        gated = proj[:, 2 * width :] * proj[:, :width]
        row = lax.broadcasted_iota(jnp.int32, gated.shape, 0)
        back1 = jnp.where(row < 1, 0.0, pltpu.roll(gated, 1, 0))
        back2 = jnp.where(row < 2, 0.0, pltpu.roll(gated, 2, 0))
        convolved = taps[0:1] * back2 + taps[1:2] * back1 + taps[2:3] * gated
        mixed = (proj[:, width : 2 * width] * convolved).astype(bf16)
        for lo in range(0, mix_cols, 1024):
            size = min(1024, mix_cols - lo)
            part[pl.ds(al(s * seq, seq), seq), pl.ds(lo, size)] = jnp.dot(
                mixed, outb[:, pl.ds(lo, size)], preferred_element_type=f32
            ).astype(bf16)
        sib_copy(0, s, part, sib, 0, mix_cols).start()

    for s in (diag[0], cross[0]):
        sib_copy(0, s, part, sib, 0, mix_cols).wait_recv()
    for n in range(far):
        reduce_x(0, n, n * group, group)
    at(6)
    for s in (pal[0], own[0]):
        sib_copy(0, s, part, sib, 0, mix_cols).wait_recv()
    for n in range(far):
        reduce_p(0, n, n * group, group)
        at(7 + n)
    for n in range(far):
        span = pl.ds(n * group, group)
        total = reduce_end(0, n, n * group, group)
        resid[:, span] = (tok_ref[:, span].astype(f32) + total).astype(bf16)
    at(11)
    slot(toks_ff, own[1], t)[...] = norm(resid[...].astype(f32), ff_gain_ref)
    ag_start(1, toks_ff)
    at(12)
    ag_relay(1, toks_ff, pal[1], (3, 4))
    at(13)
    ag_relay(1, toks_ff, cross[1], (5,))
    at(14)
    own_rest[2].wait()
    for j in range(4):
        landed(2, j, 1 - y)
    at(16)

    def up(i):
        s = seq_at(1, 3 - i)
        ag_wait(1, toks_ff, s, 1 - t)
        x = toks_ff[pl.ds(al(s * seq, seq), seq), :]
        for lo, size in ((0, 4 * unit), (4 * unit, hid - 4 * unit)):
            act = jnp.dot(x, upb[:, pl.ds(lo, size)], preferred_element_type=f32)
            hidden[pl.ds(al(s * seq, seq), seq), pl.ds(lo, size)] = jnp.square(jnp.maximum(act, 0.0)).astype(bf16)

    pl.loop(0, 3)(up)
    ag_relay(1, toks_ff, diag[1], (6,))
    at(17)
    up(3)
    at(18)

    def down(j, h):
        m = line[j] * 2 + h
        lo = al(m * cols, cols)

        @pl.loop(0, 4)
        def _(i):
            s = seq_at(1, i)
            part_ff[pl.ds(al(s * seq, seq), seq), pl.ds(lo, cols)] = jnp.dot(
                hidden[pl.ds(al(s * seq, seq), seq), pl.ds(0, hid)],
                dnb[pl.ds(0, hid), pl.ds(lo, cols)],
                preferred_element_type=f32,
            ).astype(bf16)
            sib_copy(1 + m, s, part_ff, sib_ff, lo, cols).start()

    def spread(j, h):
        m = line[j] * 2 + h
        lo = al(m * cols, cols)
        for s in (diag[1], cross[1]):
            sib_copy(1 + m, s, part_ff, sib_ff, lo, cols).wait_recv()
        reduce_x(1, far + m, lo, cols)

    def finish(j, h):
        m = line[j] * 2 + h
        lo = al(m * cols, cols)
        for s in (pal[1], own[1]):
            sib_copy(1 + m, s, part_ff, sib_ff, lo, cols).wait_recv()
        reduce_p(1, far + m, lo, cols)

    def out_copy(j, h, ys):
        span = pl.ds(al(line[j] * group + ys * cols + h * strip, strip), strip)
        return pltpu.make_async_copy(result.at[:, span], o_ref.at[:, span], out_sem.at[(j * 2 + h) * 2 + ys])

    def end(j, h):
        m = line[j] * 2 + h
        total = reduce_end(1, far + m, al(m * cols, cols), cols)
        for ys in range(2):
            span = pl.ds(al(line[j] * group + ys * cols + h * strip, strip), strip)
            result[:, span] = (resid[:, span].astype(f32) + total[:, ys * strip : (ys + 1) * strip]).astype(bf16)
            out_copy(j, h, ys).start()

    own_rest[3].wait()
    own_rest[4].wait()
    own_rest[5].wait()
    def sent_mixer():
        for k in (0, 1):
            near_copy(k).wait_send()
            for zs in range(far):
                for ys in range(2):
                    @pl.when(jnp.logical_and(zs <= z, z + 1 < far))
                    def _():
                        hop(k, zs, ys, 1, right_send).wait_send()

                    @pl.when(jnp.logical_and(zs >= z, z > 0))
                    def _():
                        hop(k, zs, ys, -1, left_send).wait_send()
        for g, buf in ((0, toks), (1, toks_ff)):
            for i in range(7):
                ag_copy(g, buf, i).wait_send()
        for s in range(4):
            sib_copy(0, s, part, sib, 0, mix_cols).wait_send()
        for n in range(far):
            lo = n * group
            for j in range(2):
                x_copy(n, j, xs, xr, lo, group).wait_send()
            p_copy(0, n, ps, pr, lo, group).wait_send()

    def sent_weights(ks):
        for k in ks:
            for i in range(3):
                w_copy(k, i).wait_send()
            for j in range(4):
                y_copy(k, j).wait_send()

    def sent_step(j, h):
        m = line[j] * 2 + h
        lo = al(m * cols, cols)
        for s in range(4):
            sib_copy(1 + m, s, part_ff, sib_ff, lo, cols).wait_send()
        for i in range(2):
            x_copy(far + m, i, xs_ff, xr_ff, lo, cols).wait_send()
        p_copy(1, far + m, ps_ff, pr_ff, lo, cols).wait_send()

    steps = [(0, 0), (0, 1), (1, 0), (1, 1), (2, 0), (3, 0), (2, 1), (3, 1)]
    late = LATE
    for n, (j, h) in enumerate(steps):
        if n >= late:
            spread(*steps[n - 1])
        if n == 6:
            sent_mixer()
        if n == 7:
            sent_weights((2,))
            for step in steps[:4]:
                sent_step(*step)
        for k in ((3,), (4, 5))[h]:
            landed(k, j, 1 - y)
        down(j, h)
        at(19 + n)
        if 0 < n < late:
            spread(*steps[n - 1])
        if n > 1:
            finish(*steps[n - 2])
        if n > 4:
            end(*steps[n - 5])
    spread(*steps[-1])
    finish(*steps[-2])
    finish(*steps[-1])
    for step in steps[-5:]:
        end(*step)

    for j, h in steps:
        for ys in range(2):
            out_copy(j, h, ys).wait()
    sent_weights((3, 4, 5))
    for step in steps[4:]:
        sent_step(*step)


def layer_kernel(far, *refs):
    z = lax.axis_index("far")
    inside = lax.rem(lax.div(z, 2) + lax.rem(z, 2), 2) == 1
    pl.when(inside)(functools.partial(chip_kernel, far, 0, *refs))
    pl.when(jnp.logical_not(inside))(functools.partial(chip_kernel, far, 1, *refs))


def fused_layer(far, tokens, mix_gain, conv_in, outer, inner, taps, out_w, ff_gain, up_w, down_w):
    bf16 = jnp.bfloat16
    rows, feat = tokens.shape
    depth, cols = up_w.shape[0], down_w.shape[1]
    width, hid = conv_in.shape[1] // 4, up_w.shape[1] * 8 // 32
    whole = 8 * rows
    vmem = pl.BlockSpec(memory_space=pltpu.VMEM)
    hbm = pl.BlockSpec(memory_space=pl.ANY)
    dma = pltpu.SemaphoreType.DMA
    block = [
        pltpu.VMEM((whole, feat), bf16),
        pltpu.VMEM((4 * rows, feat), bf16),
        pltpu.VMEM((2, rows, feat), bf16),
        pltpu.VMEM((2, rows, feat), bf16),
        pltpu.VMEM((rows, feat), bf16),
        pltpu.VMEM((rows, feat), bf16),
    ]
    return pl.pallas_call(
        functools.partial(layer_kernel, far),
        out_shape=jax.ShapeDtypeStruct((rows, feat), bf16),
        in_specs=[vmem, vmem, hbm, hbm, hbm, vmem, hbm, vmem, hbm, hbm],
        out_specs=hbm,
        scratch_shapes=[
            pltpu.VMEM((far * 2 * depth, 3 * width), bf16),
            pltpu.VMEM((width, far * 2 * cols), bf16),
            pltpu.VMEM((far * 2 * depth, hid), bf16),
            pltpu.VMEM((hid, far * 2 * cols), bf16),
            pltpu.VMEM((depth, 3 * width), bf16),
            pltpu.VMEM((whole, feat), bf16),
            pltpu.VMEM((whole, feat), bf16),
            *block,
            *block,
            pltpu.VMEM((whole, hid), bf16),
            pltpu.VMEM((rows, feat), bf16),
            pltpu.VMEM((rows, feat), bf16),
            dma((16,)),
            dma((8,)),
            dma((3,)),
            dma((2,)),
            dma((2, far * 2)),
            dma((2, far * 2)),
            dma((4, 3)),
            dma((4, 4)),
            dma((6, far * 2)),
            dma((2, 7)),
            dma((2, 8)),
            dma((1 + 2 * far, 4)),
            dma((1 + 2 * far, 4)),
            dma((3 * far, 2)),
            dma((3 * far, 2)),
            dma((3 * far,)),
            dma((3 * far,)),
        ],
        compiler_params=pltpu.CompilerParams(
            collective_id=0, has_side_effects=True, vmem_limit_bytes=60 * 2**20),
    )(tokens, mix_gain[None], conv_in, outer, inner, taps, out_w, ff_gain[None], up_w, down_w)


def solution(mesh):
    rep, fs, tp = (mesh.shape[name] for name in ("rep", "fs", "tp"))
    near = 2 if fs % 2 == 0 else 1
    mesh4 = Mesh(mesh.devices.reshape(rep, fs // near, near, tp), ("rep", "far", "near", "tp"))
    fs_axes = ("far", "near")
    rows = P(("rep", "far", "near", "tp"), None)
    in_specs = (
        rows,
        P(),
        P(fs_axes, "tp"),
        P(fs_axes, "tp"),
        P(fs_axes, "tp"),
        P(None, "tp"),
        P("tp", fs_axes),
        P(),
        P(fs_axes, "tp"),
        P("tp", fs_axes),
    )

    def body(*args):
        if rep == 2 and near == 2 and tp == 2 and fs == 8:
            return fused_layer(fs // near, *args)
        return on_device(rep, near, tp, *args)

    return jax.shard_map(body, mesh=mesh4, in_specs=in_specs, out_specs=rows, check_vma=False)
```

```python
import functools

import jax
import jax.numpy as jnp
from jax import lax
from jax.experimental import pallas as pl
from jax.experimental.pallas import tpu as pltpu
from jax.sharding import Mesh, PartitionSpec as P

eps = 1e-06


def rms_scale(values, gain):
    widened = values.astype(jnp.float32)
    inverse = lax.rsqrt(jnp.mean(widened * widened, axis=-1, keepdims=True) + eps)
    return (widened * inverse * gain).astype(jnp.bfloat16)


GROUP = ("rep", "near", "tp")


def gather_rows(block, near):
    rows, width = block.shape[0], block.shape[1] // near
    if near > 1:
        block = lax.all_to_all(
            block.reshape(rows, near, width).transpose(1, 0, 2), "near", 0, 0, tiled=True
        ).reshape(near * rows, width)
    return lax.all_gather(block, "far", axis=0, tiled=True)


def own_part(block, axis, rep):
    size = block.shape[axis] // rep
    return lax.dynamic_slice_in_dim(block, lax.axis_index("rep") * size, size, axis)


def on_device(rep, near, tp, tokens, mix_gain, conv_in, outer, inner, taps, out_w, ff_gain, up_w, down_w):
    seq_rows = tokens.shape[0] * tp
    depth = up_w.shape[0]
    parts = [own_part(w, 1, rep) for w in (conv_in, outer, inner)]
    width = parts[0].shape[1] // near
    trio = jnp.concatenate([p.reshape(depth, near, width) for p in parts], 2).reshape(depth, -1)
    trio = gather_rows(trio, near)
    out_part = own_part(out_w, 0, rep)
    out_part = out_part.reshape(near, width, -1).transpose(1, 0, 2).reshape(width, -1)
    out_full = gather_rows(out_part, near).reshape(-1, width, out_w.shape[1])
    up_full = gather_rows(own_part(up_w, 1, rep), near)
    down_part = own_part(down_w, 0, rep)
    hid = down_part.shape[0] // near
    down_part = down_part.reshape(near, hid, -1).transpose(1, 0, 2).reshape(hid, -1)
    down_full = gather_rows(down_part, near).reshape(-1, hid, down_w.shape[1])

    taps = own_part(taps, 1, rep)
    taps = lax.dynamic_slice_in_dim(taps, lax.axis_index("near") * width, width, 1)

    normed = lax.all_gather(rms_scale(tokens, mix_gain), GROUP, axis=0, tiled=True)
    proj = jnp.dot(normed, trio, preferred_element_type=jnp.float32).astype(jnp.bfloat16)
    proj = proj.astype(jnp.float32).reshape(-1, seq_rows, 3 * width)
    gated = proj[..., 2 * width :] * proj[..., :width]
    padded = jnp.pad(gated, ((0, 0), (2, 0), (0, 0)))
    convolved = sum(taps[k] * padded[:, k : seq_rows + k] for k in range(3))
    mixed = (proj[..., width : 2 * width] * convolved).astype(jnp.bfloat16)
    mixed = mixed.reshape(-1, width)

    def project(lefts, rights):
        whole = rights.transpose(1, 0, 2).reshape(lefts.shape[1], -1)
        partial = jnp.dot(lefts, whole, preferred_element_type=jnp.float32)
        return lax.psum_scatter(
            partial.astype(jnp.bfloat16), GROUP, scatter_dimension=0, tiled=True
        ).astype(jnp.float32)

    resid = (tokens.astype(jnp.float32) + project(mixed, out_full)).astype(jnp.bfloat16)
    normed_ff = lax.all_gather(rms_scale(resid, ff_gain), GROUP, axis=0, tiled=True)
    preact = jnp.dot(normed_ff, up_full, preferred_element_type=jnp.float32)
    hidden = jnp.square(jax.nn.relu(preact)).astype(jnp.bfloat16)
    return (resid.astype(jnp.float32) + project(hidden, down_full)).astype(jnp.bfloat16)


SEND, OWN, TAKE, LEND, PASS = range(5)
LATE = 6
PLAN = (
    {
        2: ((OWN, 2, 0), (OWN, 3, 0), (OWN, 4, 0), (OWN, 5, 0),),
        4: ((SEND, 2, 1), (SEND, 2, 0),),
        5: ((TAKE, 2, 1),),
        7: ((SEND, 2, 2),),
        10: ((TAKE, 2, 2), (TAKE, 2, 3),),
        12: ((SEND, 3, 0), (SEND, 3, 1), (SEND, 3, 2), (SEND, 4, 1), (SEND, 5, 1), (SEND, 4, 2), (SEND, 5, 2), (SEND, 4, 0), (SEND, 5, 0), (TAKE, 3, 1), (TAKE, 4, 1), (TAKE, 5, 1),),
        14: ((TAKE, 3, 2),),
        16: ((TAKE, 3, 3),),
        21: ((TAKE, 4, 2),),
        22: ((TAKE, 5, 2), (TAKE, 4, 3),),
        23: ((TAKE, 5, 3),),
    },
    {
        1: ((LEND, 0, 0), (SEND, 2, 0),),
        2: ((OWN, 2, 0), (OWN, 3, 0), (OWN, 4, 0), (OWN, 5, 0),),
        3: ((SEND, 2, 2), (PASS, 0, 0), (SEND, 3, 0), (SEND, 4, 0), (SEND, 5, 0),),
        6: ((TAKE, 2, 1), (SEND, 2, 1),),
        12: ((TAKE, 2, 2), (TAKE, 2, 3), (SEND, 3, 2), (SEND, 3, 1),),
        13: ((SEND, 4, 2), (SEND, 5, 2), (SEND, 4, 1), (SEND, 5, 1),),
        14: ((TAKE, 3, 1),),
        16: ((TAKE, 3, 2),),
        17: ((TAKE, 3, 3),),
        18: ((TAKE, 4, 1),),
        19: ((TAKE, 5, 1),),
        20: ((TAKE, 4, 2),),
        21: ((TAKE, 5, 2),),
        22: ((TAKE, 4, 3),),
        23: ((TAKE, 5, 3),),
    },
)
STEPS = (
    ((0, 0), (0, 1), (1, 0), (1, 1), (2, 0), (3, 0), (2, 1), (3, 1)),
    ((0, 0), (0, 1), (1, 0), (2, 0), (3, 0), (1, 1), (2, 1), (3, 1)),
)


def visit_order(far):
    return [sorted(range(far), key=lambda s: (abs(s - z), s)) for z in range(far)]


def chip_kernel(
    far, edge,
    tok_ref, mix_gain_ref, conv_ref, outer_ref, inner_ref, taps_ref, outw_ref, ff_gain_ref, upw_ref, dnw_ref,
    o_ref,
    trio, outb, upb, dnb, stage, toks, toks_ff,
    part, sib, xs, xr, ps, pr, part_ff, sib_ff, xs_ff, xr_ff, ps_ff, pr_ff,
    hidden, resid, result, out_sem, swap, swap_sem,
    local_sem, stage_sem, near_send, right_send, left_send, w_send, y_send, w_recv,
    ag_send, ag_recv, sib_send, sib_recv, x_send, x_recv, p_send, p_recv,
):
    r, z, y, t = (lax.axis_index(name) for name in ("rep", "far", "near", "tp"))
    rows = tok_ref.shape[0]
    seq = 2 * rows
    width = trio.shape[1] // 3
    depth = upw_ref.shape[0]
    unit = upw_ref.shape[1] // 32
    sizes = (9 * unit, 7 * unit)
    hid = sizes[edge]
    cols = dnw_ref.shape[1]
    group, strip = 2 * cols, cols // 2
    bf16, f32 = jnp.bfloat16, jnp.float32

    half_z = lax.rem(z, 2)
    zp = z + 1 - 2 * half_z
    zm = far - 1 - z
    zd = far - 1 - zp
    line = (z, zp, zm, zd)
    side = (y, half_z)
    own, cross, pal, diag = (
        [rr * 2 + ee for ee in ends]
        for rr, ends in ((r, side), (1 - r, side), (r, (1 - y, 1 - half_z)), (1 - r, (1 - y, 1 - half_z)))
    )

    def split(kind):
        return pl.ds(al(r * 16 * unit + kind * sizes[0], unit), sizes[kind])

    sibling = (r, z, y, 1 - t)
    beside = (r, z, 1 - y, t)
    across = (1 - r, z, y, t)
    partner = (beside, (r, zp, y, t))

    def al(v, n):
        return pl.multiple_of(v, n)

    def push(a, b, s, q, where):
        return pltpu.make_async_remote_copy(
            src_ref=a, dst_ref=b, send_sem=s, recv_sem=q, device_id=where, device_id_type=pl.DeviceIdType.MESH
        )

    def lines(k, size):
        half = size // (2 * unit) * unit
        return ((0, size), (0, half), (half, size - half))[k - 3]

    def place(k, zs, ys, kind=None):
        p = zs * 2 + ys
        if k == 0:
            return trio.at[pl.ds(al(p * depth, depth), depth), :]
        if k == 1:
            return outb.at[:, pl.ds(al(p * cols, cols), cols)]
        size = sizes[edge if kind is None else kind]
        if k == 2:
            return upb.at[pl.ds(al(p * depth, depth), depth), pl.ds(0, size)]
        lo = ((zs * 2 + min(k - 3, 1)) * 2 + ys) * strip
        top, some = lines(k, size)
        return dnb.at[pl.ds(top, some), pl.ds(al(lo, strip), strip)]

    def share(k, q):
        if k == 1:
            return outw_ref.at[pl.ds(al(q * width, width), width), :]
        if k == 2:
            return upw_ref.at[:, split(q)]
        top, some = lines(k, sizes[q])
        start = al(r * 16 * unit + q * sizes[0] + top, unit)
        return dnw_ref.at[pl.ds(start, some), pl.ds(min(k - 3, 1) * strip, strip)]

    def trio_copies(dst, q, sems):
        return [
            pltpu.make_async_copy(
                w.at[:, pl.ds(al(q * width, width), width)],
                dst.at[:, pl.ds(j * width, width)],
                sems.at[j],
            )
            for j, w in enumerate((conv_ref, outer_ref, inner_ref))
        ]

    own_trio = trio_copies(place(0, z, y), r * 2 + y, local_sem)
    other_trio = trio_copies(stage, r * 2 + 1 - y, stage_sem)
    own_rest = [None] + [
        pltpu.make_async_copy(share(k, r * 2 + y if k == 1 else edge), place(k, z, y), local_sem.at[2 + k])
        for k in (1, 2, 3, 4, 5)
    ]

    def near_copy(k):
        a = stage if k == 0 else share(k, r * 2 + 1 - y)
        return push(a, place(k, z, y), near_send.at[k], w_recv.at[k, z * 2 + y], beside)

    def hop(k, zs, ys, step, sems):
        p = zs * 2 + ys
        at = place(k, zs, ys)
        return push(at, at, sems.at[k, p], w_recv.at[k, p], (r, z + step, y, t))

    order = visit_order(far)

    def nth(j):
        zs = jnp.int32(order[0][j])
        for c in range(1, far):
            zs = jnp.where(z == c, order[c][j], zs)
        return zs

    def send_on(k, zs, ys):
        @pl.when(jnp.logical_and(zs <= z, z + 1 < far))
        def _():
            hop(k, zs, ys, 1, right_send).start()

        @pl.when(jnp.logical_and(zs >= z, z > 0))
        def _():
            hop(k, zs, ys, -1, left_send).start()

    def mix_landed(k, zs, ys):
        at = place(k, zs, ys)
        push(at, at, near_send.at[k], w_recv.at[k, zs * 2 + ys], beside).wait_recv()
        send_on(k, zs, ys)

    def w_copy(k, i):
        kind = edge if i == 1 else 1 - edge
        return push(
            share(k, kind), place(k, z, y, kind), w_send.at[k - 2, i], w_recv.at[k, z * 2 + y], (r, (zp, zm, zd)[i], y, t)
        )

    def y_copy(k, j):
        at = place(k, line[j], y)
        a = share(k, edge) if j == 0 else at
        return push(a, at, y_send.at[k - 2, j], w_recv.at[k, line[j] * 2 + y], beside)

    def landed(k, j, ys):
        at = place(k, line[j], ys)
        push(at, at, y_send.at[k - 2, j], w_recv.at[k, line[j] * 2 + ys], beside).wait_recv()

    def through(k, j):
        return edge == 0 and k == 2 and j == 1

    def arrive(k, j):
        landed(k, j, y)
        if not through(k, j):
            y_copy(k, j).start()

    def lend():
        return push(share(2, 0), swap, swap_sem.at[0], swap_sem.at[1], beside)

    def lent():
        return push(swap, place(2, z, 1 - y, 0), swap_sem.at[2], w_recv.at[2, z * 2 + 1 - y], partner[1])

    def at(point):
        for what, k, i in PLAN[edge].get(point, ()):
            if what == SEND:
                w_copy(k, i).start()
            elif what == OWN:
                y_copy(k, 0).start()
            elif what == TAKE:
                arrive(k, i)
            elif what == LEND:
                lend().start()
            else:
                lend().wait_recv()
                lent().start()

    def norm(values, gain_ref):
        inverse = lax.rsqrt(jnp.mean(values * values, axis=-1, keepdims=True) + eps)
        return (values * inverse * gain_ref[...]).astype(bf16)

    def slot(buf, s, core):
        return buf.at[pl.ds(al((s * 2 + core) * rows, rows), rows), :]

    def ag_copy(g, buf, i):
        s, core, where = (
            (own[g], t, partner[g]), (own[g], t, across), (own[g], t, sibling),
            (pal[g], t, across), (pal[g], t, sibling), (cross[g], t, sibling), (diag[g], t, sibling),
        )[i]
        at = slot(buf, s, core)
        return push(at, at, ag_send.at[g, i], ag_recv.at[g, s * 2 + core], where)

    def ag_wait(g, buf, s, core):
        at = slot(buf, s, core)
        push(at, at, ag_send.at[g, 0], ag_recv.at[g, s * 2 + core], sibling).wait_recv()

    def ag_start(g, buf):
        for i in range(3):
            ag_copy(g, buf, i).start()

    def ag_relay(g, buf, s, sends):
        ag_wait(g, buf, s, t)
        for i in sends:
            ag_copy(g, buf, i).start()

    def sib_copy(n, s, buf, land, lo, size):
        at = buf.at[pl.ds(al(s * seq + (1 - t) * rows, rows), rows), pl.ds(lo, size)]
        to = land.at[pl.ds(al(s * rows, rows), rows), pl.ds(lo, size)]
        return push(at, to, sib_send.at[n, s], sib_recv.at[n, s], sibling)

    def x_copy(n, j, send, land, lo, size):
        return push(
            send.at[j, :, pl.ds(lo, size)], land.at[j, :, pl.ds(lo, size)], x_send.at[n, j], x_recv.at[n, j], across
        )

    def p_copy(g, n, send, land, lo, size):
        return push(send.at[:, pl.ds(lo, size)], land.at[:, pl.ds(lo, size)], p_send.at[n], p_recv.at[n], partner[g])

    def both(s, buf, land, lo, size):
        return (
            buf[pl.ds(al(s * seq + t * rows, rows), rows), pl.ds(lo, size)].astype(f32)
            + land[pl.ds(al(s * rows, rows), rows), pl.ds(lo, size)].astype(f32)
        )

    mixer = (part, sib, xs, xr, ps, pr)
    ff = (part_ff, sib_ff, xs_ff, xr_ff, ps_ff, pr_ff)

    def reduce_x(g, n, lo, size):
        buf, land, send, xland, _, _ = (mixer, ff)[g]
        for j, s in ((0, diag[g]), (1, cross[g])):
            send[j, :, pl.ds(lo, size)] = both(s, buf, land, lo, size).astype(bf16)
            x_copy(n, j, send, xland, lo, size).start()

    def reduce_p(g, n, lo, size):
        buf, land, send, xland, psend, pland = (mixer, ff)[g]
        x_copy(n, 0, send, xland, lo, size).wait_recv()
        total = both(pal[g], buf, land, lo, size) + xland[0, :, pl.ds(lo, size)].astype(f32)
        psend[:, pl.ds(lo, size)] = total.astype(bf16)
        p_copy(g, n, psend, pland, lo, size).start()

    def reduce_end(g, n, lo, size):
        buf, land, send, xland, psend, pland = (mixer, ff)[g]
        x_copy(n, 1, send, xland, lo, size).wait_recv()
        p_copy(g, n, psend, pland, lo, size).wait_recv()
        return (
            both(own[g], buf, land, lo, size)
            + xland[1, :, pl.ds(lo, size)].astype(f32)
            + pland[:, pl.ds(lo, size)].astype(f32)
        )

    def seq_at(g, i):
        rr = lax.rem(r + 1 + lax.div(i, 2), 2)
        ee = lax.rem(side[g] + 1 + lax.rem(i, 2), 2)
        return rr * 2 + ee

    barrier = pltpu.get_barrier_semaphore()
    peers = (sibling, beside, across, partner[1], (r, zm, y, t), (r, zd, y, t))
    for where in peers:
        pl.semaphore_signal(barrier, inc=1, device_id=where, device_id_type=pl.DeviceIdType.MESH)
    for copy in other_trio + own_trio + own_rest[1:]:
        copy.start()
    slot(toks, own[0], t)[...] = norm(tok_ref[...].astype(f32), mix_gain_ref)
    pl.semaphore_wait(barrier, len(peers))
    for copy in other_trio:
        copy.wait()
    near_copy(0).start()
    near_copy(1).start()
    for copy in own_trio:
        copy.wait()
    send_on(0, z, y)
    own_rest[1].wait()
    send_on(1, z, y)
    ag_start(0, toks)
    at(0)
    for k in (0, 1):
        mix_landed(k, z, 1 - y)
    at(1)
    for k in (0, 1):
        for ys in (y, 1 - y):
            mix_landed(k, nth(1), ys)
    at(2)
    for k in (0, 1):
        for ys in (y, 1 - y):
            mix_landed(k, nth(2), ys)
    at(3)
    ag_relay(0, toks, pal[0], (3, 4))
    ag_relay(0, toks, cross[0], (5,))
    for k in (0, 1):
        for ys in (y, 1 - y):
            mix_landed(k, nth(3), ys)
    at(4)
    ag_relay(0, toks, diag[0], (6,))
    for s in (own[0], cross[0], pal[0], diag[0]):
        ag_wait(0, toks, s, 1 - t)
    at(5)

    mix_cols = outb.shape[1]
    taps = taps_ref[:, pl.ds(al((r * 2 + y) * width, width), width)]

    @pl.loop(0, 4)
    def _(i):
        s = seq_at(0, i)
        x = toks[pl.ds(al(s * seq, seq), seq), :]
        proj = jnp.dot(x, trio[...], preferred_element_type=f32).astype(bf16).astype(f32)
        gated = proj[:, 2 * width :] * proj[:, :width]
        row = lax.broadcasted_iota(jnp.int32, gated.shape, 0)
        back1 = jnp.where(row < 1, 0.0, pltpu.roll(gated, 1, 0))
        back2 = jnp.where(row < 2, 0.0, pltpu.roll(gated, 2, 0))
        convolved = taps[0:1] * back2 + taps[1:2] * back1 + taps[2:3] * gated
        mixed = (proj[:, width : 2 * width] * convolved).astype(bf16)
        for lo in range(0, mix_cols, 1024):
            size = min(1024, mix_cols - lo)
            part[pl.ds(al(s * seq, seq), seq), pl.ds(lo, size)] = jnp.dot(
                mixed, outb[:, pl.ds(lo, size)], preferred_element_type=f32
            ).astype(bf16)
        sib_copy(0, s, part, sib, 0, mix_cols).start()

    for s in (diag[0], cross[0]):
        sib_copy(0, s, part, sib, 0, mix_cols).wait_recv()
    for n in range(far):
        reduce_x(0, n, n * group, group)
    at(6)
    for s in (pal[0], own[0]):
        sib_copy(0, s, part, sib, 0, mix_cols).wait_recv()
    for n in range(far):
        reduce_p(0, n, n * group, group)
        at(7 + n)
    for n in range(far):
        span = pl.ds(n * group, group)
        total = reduce_end(0, n, n * group, group)
        resid[:, span] = (tok_ref[:, span].astype(f32) + total).astype(bf16)
    at(11)
    slot(toks_ff, own[1], t)[...] = norm(resid[...].astype(f32), ff_gain_ref)
    ag_start(1, toks_ff)
    at(12)
    ag_relay(1, toks_ff, pal[1], (3, 4))
    at(13)
    ag_relay(1, toks_ff, cross[1], (5,))
    at(14)
    own_rest[2].wait()
    for j in range(4):
        landed(2, j, 1 - y)
    at(16)

    def up(i):
        s = seq_at(1, 3 - i)
        ag_wait(1, toks_ff, s, 1 - t)
        x = toks_ff[pl.ds(al(s * seq, seq), seq), :]
        for lo, size in ((0, 4 * unit), (4 * unit, hid - 4 * unit)):
            act = jnp.dot(x, upb[:, pl.ds(lo, size)], preferred_element_type=f32)
            hidden[pl.ds(al(s * seq, seq), seq), pl.ds(lo, size)] = jnp.square(jnp.maximum(act, 0.0)).astype(bf16)

    pl.loop(0, 3)(up)
    ag_relay(1, toks_ff, diag[1], (6,))
    at(17)
    up(3)
    at(18)

    def down(j, h):
        m = line[j] * 2 + h
        lo = al(m * cols, cols)

        @pl.loop(0, 4)
        def _(i):
            s = seq_at(1, i)
            part_ff[pl.ds(al(s * seq, seq), seq), pl.ds(lo, cols)] = jnp.dot(
                hidden[pl.ds(al(s * seq, seq), seq), pl.ds(0, hid)],
                dnb[pl.ds(0, hid), pl.ds(lo, cols)],
                preferred_element_type=f32,
            ).astype(bf16)
            sib_copy(1 + m, s, part_ff, sib_ff, lo, cols).start()

    def spread(j, h):
        m = line[j] * 2 + h
        lo = al(m * cols, cols)
        for s in (diag[1], cross[1]):
            sib_copy(1 + m, s, part_ff, sib_ff, lo, cols).wait_recv()
        reduce_x(1, far + m, lo, cols)

    def finish(j, h):
        m = line[j] * 2 + h
        lo = al(m * cols, cols)
        for s in (pal[1], own[1]):
            sib_copy(1 + m, s, part_ff, sib_ff, lo, cols).wait_recv()
        reduce_p(1, far + m, lo, cols)

    def out_copy(j, h, ys):
        span = pl.ds(al(line[j] * group + ys * cols + h * strip, strip), strip)
        return pltpu.make_async_copy(result.at[:, span], o_ref.at[:, span], out_sem.at[(j * 2 + h) * 2 + ys])

    def end(j, h):
        m = line[j] * 2 + h
        total = reduce_end(1, far + m, al(m * cols, cols), cols)
        for ys in range(2):
            span = pl.ds(al(line[j] * group + ys * cols + h * strip, strip), strip)
            result[:, span] = (resid[:, span].astype(f32) + total[:, ys * strip : (ys + 1) * strip]).astype(bf16)
            out_copy(j, h, ys).start()

    own_rest[3].wait()
    own_rest[4].wait()
    own_rest[5].wait()
    def sent_mixer():
        for k in (0, 1):
            near_copy(k).wait_send()
            for zs in range(far):
                for ys in range(2):
                    @pl.when(jnp.logical_and(zs <= z, z + 1 < far))
                    def _():
                        hop(k, zs, ys, 1, right_send).wait_send()

                    @pl.when(jnp.logical_and(zs >= z, z > 0))
                    def _():
                        hop(k, zs, ys, -1, left_send).wait_send()
        for g, buf in ((0, toks), (1, toks_ff)):
            for i in range(7):
                ag_copy(g, buf, i).wait_send()
        for s in range(4):
            sib_copy(0, s, part, sib, 0, mix_cols).wait_send()
        for n in range(far):
            lo = n * group
            for j in range(2):
                x_copy(n, j, xs, xr, lo, group).wait_send()
            p_copy(0, n, ps, pr, lo, group).wait_send()

    def sent_weights(ks):
        for k in ks:
            for i in range(3):
                w_copy(k, i).wait_send()
            for j in range(4):
                if not through(k, j):
                    y_copy(k, j).wait_send()

    def sent_step(j, h):
        m = line[j] * 2 + h
        lo = al(m * cols, cols)
        for s in range(4):
            sib_copy(1 + m, s, part_ff, sib_ff, lo, cols).wait_send()
        for i in range(2):
            x_copy(far + m, i, xs_ff, xr_ff, lo, cols).wait_send()
        p_copy(1, far + m, ps_ff, pr_ff, lo, cols).wait_send()

    steps = STEPS[edge]
    late = LATE
    for n, (j, h) in enumerate(steps):
        if n >= late:
            spread(*steps[n - 1])
        if n == 6:
            sent_mixer()
        if n == 7:
            sent_weights((2,))
            for step in steps[:4]:
                sent_step(*step)
        for k in ((3,), (4, 5))[h]:
            landed(k, j, 1 - y)
        down(j, h)
        at(19 + n)
        if 0 < n < late:
            spread(*steps[n - 1])
        if n > 1:
            finish(*steps[n - 2])
    spread(*steps[-1])
    finish(*steps[-2])
    finish(*steps[-1])
    for step in steps:
        end(*step)

    for j, h in steps:
        for ys in range(2):
            out_copy(j, h, ys).wait()
    sent_weights((3, 4, 5))
    if edge == 1:
        lend().wait_send()
        lent().wait_send()
    for step in steps[4:]:
        sent_step(*step)


def layer_kernel(far, *refs):
    z = lax.axis_index("far")
    inside = lax.rem(lax.div(z, 2) + lax.rem(z, 2), 2) == 1
    pl.when(inside)(functools.partial(chip_kernel, far, 0, *refs))
    pl.when(jnp.logical_not(inside))(functools.partial(chip_kernel, far, 1, *refs))


def fused_layer(far, tokens, mix_gain, conv_in, outer, inner, taps, out_w, ff_gain, up_w, down_w):
    bf16 = jnp.bfloat16
    rows, feat = tokens.shape
    depth, cols = up_w.shape[0], down_w.shape[1]
    width, hid = conv_in.shape[1] // 4, up_w.shape[1] * 9 // 32
    whole = 8 * rows
    vmem = pl.BlockSpec(memory_space=pltpu.VMEM)
    hbm = pl.BlockSpec(memory_space=pl.ANY)
    dma = pltpu.SemaphoreType.DMA
    block = [
        pltpu.VMEM((whole, feat), bf16),
        pltpu.VMEM((4 * rows, feat), bf16),
        pltpu.VMEM((2, rows, feat), bf16),
        pltpu.VMEM((2, rows, feat), bf16),
        pltpu.VMEM((rows, feat), bf16),
        pltpu.VMEM((rows, feat), bf16),
    ]
    return pl.pallas_call(
        functools.partial(layer_kernel, far),
        out_shape=jax.ShapeDtypeStruct((rows, feat), bf16),
        in_specs=[vmem, vmem, hbm, hbm, hbm, vmem, hbm, vmem, hbm, hbm],
        out_specs=hbm,
        scratch_shapes=[
            pltpu.VMEM((far * 2 * depth, 3 * width), bf16),
            pltpu.VMEM((width, far * 2 * cols), bf16),
            pltpu.VMEM((far * 2 * depth, hid), bf16),
            pltpu.VMEM((hid, far * 2 * cols), bf16),
            pltpu.VMEM((depth, 3 * width), bf16),
            pltpu.VMEM((whole, feat), bf16),
            pltpu.VMEM((whole, feat), bf16),
            *block,
            *block,
            pltpu.VMEM((whole, hid), bf16),
            pltpu.VMEM((rows, feat), bf16),
            pltpu.VMEM((rows, feat), bf16),
            dma((16,)),
            pltpu.VMEM((depth, hid), bf16),
            dma((3,)),
            dma((8,)),
            dma((3,)),
            dma((2,)),
            dma((2, far * 2)),
            dma((2, far * 2)),
            dma((4, 3)),
            dma((4, 4)),
            dma((6, far * 2)),
            dma((2, 7)),
            dma((2, 8)),
            dma((1 + 2 * far, 4)),
            dma((1 + 2 * far, 4)),
            dma((3 * far, 2)),
            dma((3 * far, 2)),
            dma((3 * far,)),
            dma((3 * far,)),
        ],
        compiler_params=pltpu.CompilerParams(
            collective_id=0, has_side_effects=True, vmem_limit_bytes=60 * 2**20),
    )(tokens, mix_gain[None], conv_in, outer, inner, taps, out_w, ff_gain[None], up_w, down_w)


def solution(mesh):
    rep, fs, tp = (mesh.shape[name] for name in ("rep", "fs", "tp"))
    near = 2 if fs % 2 == 0 else 1
    mesh4 = Mesh(mesh.devices.reshape(rep, fs // near, near, tp), ("rep", "far", "near", "tp"))
    fs_axes = ("far", "near")
    rows = P(("rep", "far", "near", "tp"), None)
    in_specs = (
        rows,
        P(),
        P(fs_axes, "tp"),
        P(fs_axes, "tp"),
        P(fs_axes, "tp"),
        P(None, "tp"),
        P("tp", fs_axes),
        P(),
        P(fs_axes, "tp"),
        P("tp", fs_axes),
    )

    def body(*args):
        if rep == 2 and near == 2 and tp == 2 and fs == 8:
            return fused_layer(fs // near, *args)
        return on_device(rep, near, tp, *args)

    return jax.shard_map(body, mesh=mesh4, in_specs=in_specs, out_specs=rows, check_vma=False)
```

```python
import functools

import jax
import jax.numpy as jnp
from jax import lax
from jax.experimental import pallas as pl
from jax.experimental.pallas import tpu as pltpu
from jax.sharding import Mesh, PartitionSpec as P

eps = 1e-06


def rms_scale(values, gain):
    widened = values.astype(jnp.float32)
    inverse = lax.rsqrt(jnp.mean(widened * widened, axis=-1, keepdims=True) + eps)
    return (widened * inverse * gain).astype(jnp.bfloat16)


GROUP = ("rep", "near", "tp")


def gather_rows(block, near):
    rows, width = block.shape[0], block.shape[1] // near
    if near > 1:
        block = lax.all_to_all(
            block.reshape(rows, near, width).transpose(1, 0, 2), "near", 0, 0, tiled=True
        ).reshape(near * rows, width)
    return lax.all_gather(block, "far", axis=0, tiled=True)


def own_part(block, axis, rep):
    size = block.shape[axis] // rep
    return lax.dynamic_slice_in_dim(block, lax.axis_index("rep") * size, size, axis)


def on_device(rep, near, tp, tokens, mix_gain, conv_in, outer, inner, taps, out_w, ff_gain, up_w, down_w):
    seq_rows = tokens.shape[0] * tp
    depth = up_w.shape[0]
    parts = [own_part(w, 1, rep) for w in (conv_in, outer, inner)]
    width = parts[0].shape[1] // near
    trio = jnp.concatenate([p.reshape(depth, near, width) for p in parts], 2).reshape(depth, -1)
    trio = gather_rows(trio, near)
    out_part = own_part(out_w, 0, rep)
    out_part = out_part.reshape(near, width, -1).transpose(1, 0, 2).reshape(width, -1)
    out_full = gather_rows(out_part, near).reshape(-1, width, out_w.shape[1])
    up_full = gather_rows(own_part(up_w, 1, rep), near)
    down_part = own_part(down_w, 0, rep)
    hid = down_part.shape[0] // near
    down_part = down_part.reshape(near, hid, -1).transpose(1, 0, 2).reshape(hid, -1)
    down_full = gather_rows(down_part, near).reshape(-1, hid, down_w.shape[1])

    taps = own_part(taps, 1, rep)
    taps = lax.dynamic_slice_in_dim(taps, lax.axis_index("near") * width, width, 1)

    normed = lax.all_gather(rms_scale(tokens, mix_gain), GROUP, axis=0, tiled=True)
    proj = jnp.dot(normed, trio, preferred_element_type=jnp.float32).astype(jnp.bfloat16)
    proj = proj.astype(jnp.float32).reshape(-1, seq_rows, 3 * width)
    gated = proj[..., 2 * width :] * proj[..., :width]
    padded = jnp.pad(gated, ((0, 0), (2, 0), (0, 0)))
    convolved = sum(taps[k] * padded[:, k : seq_rows + k] for k in range(3))
    mixed = (proj[..., width : 2 * width] * convolved).astype(jnp.bfloat16)
    mixed = mixed.reshape(-1, width)

    def project(lefts, rights):
        whole = rights.transpose(1, 0, 2).reshape(lefts.shape[1], -1)
        partial = jnp.dot(lefts, whole, preferred_element_type=jnp.float32)
        return lax.psum_scatter(
            partial.astype(jnp.bfloat16), GROUP, scatter_dimension=0, tiled=True
        ).astype(jnp.float32)

    resid = (tokens.astype(jnp.float32) + project(mixed, out_full)).astype(jnp.bfloat16)
    normed_ff = lax.all_gather(rms_scale(resid, ff_gain), GROUP, axis=0, tiled=True)
    preact = jnp.dot(normed_ff, up_full, preferred_element_type=jnp.float32)
    hidden = jnp.square(jax.nn.relu(preact)).astype(jnp.bfloat16)
    return (resid.astype(jnp.float32) + project(hidden, down_full)).astype(jnp.bfloat16)


SEND, OWN, TAKE, LEND, PASS = range(5)
LATE = 6
PLAN = (
    {
        2: ((OWN, 2, 0), (OWN, 3, 0), (OWN, 4, 0), (OWN, 5, 0),),
        4: ((SEND, 2, 1), (SEND, 2, 0),),
        5: ((TAKE, 2, 1),),
        7: ((SEND, 2, 2),),
        10: ((TAKE, 2, 2), (TAKE, 2, 3),),
        12: ((SEND, 3, 0), (SEND, 3, 1), (SEND, 3, 2), (SEND, 4, 1), (SEND, 5, 1), (SEND, 4, 2), (SEND, 5, 2), (SEND, 4, 0), (SEND, 5, 0), (TAKE, 3, 1), (TAKE, 4, 1), (TAKE, 5, 1),),
        14: ((TAKE, 3, 2),),
        16: ((TAKE, 3, 3),),
        21: ((TAKE, 4, 2),),
        22: ((TAKE, 5, 2), (TAKE, 4, 3),),
        23: ((TAKE, 5, 3),),
    },
    {
        1: ((LEND, 0, 0), (SEND, 2, 0),),
        2: ((OWN, 2, 0), (OWN, 3, 0), (OWN, 4, 0), (OWN, 5, 0),),
        3: ((SEND, 2, 2), (PASS, 0, 0), (SEND, 3, 0), (SEND, 4, 0), (SEND, 5, 0),),
        6: ((TAKE, 2, 1), (SEND, 2, 1),),
        11: ((TAKE, 2, 2),),
        12: ((TAKE, 2, 3), (SEND, 3, 2), (SEND, 3, 1),),
        13: ((SEND, 4, 2), (SEND, 5, 2), (SEND, 4, 1), (SEND, 5, 1),),
        14: ((TAKE, 3, 1),),
        16: ((TAKE, 3, 2),),
        17: ((TAKE, 3, 3),),
        18: ((TAKE, 4, 1),),
        19: ((TAKE, 5, 1),),
        20: ((TAKE, 4, 2),),
        21: ((TAKE, 5, 2),),
        22: ((TAKE, 4, 3),),
        23: ((TAKE, 5, 3),),
    },
)
STEPS = (
    ((0, 0), (0, 1), (1, 0), (1, 1), (2, 0), (3, 0), (2, 1), (3, 1)),
    ((0, 0), (0, 1), (1, 0), (2, 0), (3, 0), (1, 1), (2, 1), (3, 1)),
)


def visit_order(far):
    return [sorted(range(far), key=lambda s: (abs(s - z), s)) for z in range(far)]


def chip_kernel(
    far, edge,
    tok_ref, mix_gain_ref, conv_ref, outer_ref, inner_ref, taps_ref, outw_ref, ff_gain_ref, upw_ref, dnw_ref,
    o_ref,
    trio, outb, upb, dnb, stage, toks, toks_ff,
    part, sib, xs, xr, ps, pr, part_ff, sib_ff, xs_ff, xr_ff, ps_ff, pr_ff,
    hidden, resid, result, out_sem, swap, swap_sem,
    local_sem, stage_sem, near_send, right_send, left_send, w_send, y_send, w_recv,
    ag_send, ag_recv, sib_send, sib_recv, x_send, x_recv, p_send, p_recv,
):
    r, z, y, t = (lax.axis_index(name) for name in ("rep", "far", "near", "tp"))
    rows = tok_ref.shape[0]
    seq = 2 * rows
    width = trio.shape[1] // 3
    depth = upw_ref.shape[0]
    unit = upw_ref.shape[1] // 32
    sizes = (9 * unit, 7 * unit)
    hid = sizes[edge]
    cols = dnw_ref.shape[1]
    group, strip = 2 * cols, cols // 2
    bf16, f32 = jnp.bfloat16, jnp.float32

    half_z = lax.rem(z, 2)
    zp = z + 1 - 2 * half_z
    zm = far - 1 - z
    zd = far - 1 - zp
    line = (z, zp, zm, zd)
    side = (y, half_z)
    own, cross, pal, diag = (
        [rr * 2 + ee for ee in ends]
        for rr, ends in ((r, side), (1 - r, side), (r, (1 - y, 1 - half_z)), (1 - r, (1 - y, 1 - half_z)))
    )

    def split(kind):
        return pl.ds(al(r * 16 * unit + kind * sizes[0], unit), sizes[kind])

    sibling = (r, z, y, 1 - t)
    beside = (r, z, 1 - y, t)
    across = (1 - r, z, y, t)
    partner = (beside, (r, zp, y, t))

    def al(v, n):
        return pl.multiple_of(v, n)

    def push(a, b, s, q, where):
        return pltpu.make_async_remote_copy(
            src_ref=a, dst_ref=b, send_sem=s, recv_sem=q, device_id=where, device_id_type=pl.DeviceIdType.MESH
        )

    def lines(k, size):
        half = size // (2 * unit) * unit
        return ((0, size), (0, half), (half, size - half))[k - 3]

    def place(k, zs, ys, kind=None):
        p = zs * 2 + ys
        if k == 0:
            return trio.at[pl.ds(al(p * depth, depth), depth), :]
        if k == 1:
            return outb.at[:, pl.ds(al(p * cols, cols), cols)]
        size = sizes[edge if kind is None else kind]
        if k == 2:
            return upb.at[pl.ds(al(p * depth, depth), depth), pl.ds(0, size)]
        lo = ((zs * 2 + min(k - 3, 1)) * 2 + ys) * strip
        top, some = lines(k, size)
        return dnb.at[pl.ds(top, some), pl.ds(al(lo, strip), strip)]

    def share(k, q):
        if k == 1:
            return outw_ref.at[pl.ds(al(q * width, width), width), :]
        if k == 2:
            return upw_ref.at[:, split(q)]
        top, some = lines(k, sizes[q])
        start = al(r * 16 * unit + q * sizes[0] + top, unit)
        return dnw_ref.at[pl.ds(start, some), pl.ds(min(k - 3, 1) * strip, strip)]

    def trio_copies(dst, q, sems):
        return [
            pltpu.make_async_copy(
                w.at[:, pl.ds(al(q * width, width), width)],
                dst.at[:, pl.ds(j * width, width)],
                sems.at[j],
            )
            for j, w in enumerate((conv_ref, outer_ref, inner_ref))
        ]

    own_trio = trio_copies(place(0, z, y), r * 2 + y, local_sem)
    other_trio = trio_copies(stage, r * 2 + 1 - y, stage_sem)
    own_rest = [None] + [
        pltpu.make_async_copy(share(k, r * 2 + y if k == 1 else edge), place(k, z, y), local_sem.at[2 + k])
        for k in (1, 2, 3, 4, 5)
    ]

    def near_copy(k):
        a = stage if k == 0 else share(k, r * 2 + 1 - y)
        return push(a, place(k, z, y), near_send.at[k], w_recv.at[k, z * 2 + y], beside)

    def hop(k, zs, ys, step, sems):
        p = zs * 2 + ys
        at = place(k, zs, ys)
        return push(at, at, sems.at[k, p], w_recv.at[k, p], (r, z + step, y, t))

    order = visit_order(far)

    def nth(j):
        zs = jnp.int32(order[0][j])
        for c in range(1, far):
            zs = jnp.where(z == c, order[c][j], zs)
        return zs

    def send_on(k, zs, ys):
        @pl.when(jnp.logical_and(zs <= z, z + 1 < far))
        def _():
            hop(k, zs, ys, 1, right_send).start()

        @pl.when(jnp.logical_and(zs >= z, z > 0))
        def _():
            hop(k, zs, ys, -1, left_send).start()

    def mix_landed(k, zs, ys):
        at = place(k, zs, ys)
        push(at, at, near_send.at[k], w_recv.at[k, zs * 2 + ys], beside).wait_recv()
        send_on(k, zs, ys)

    def w_copy(k, i):
        kind = edge if i == 1 else 1 - edge
        return push(
            share(k, kind), place(k, z, y, kind), w_send.at[k - 2, i], w_recv.at[k, z * 2 + y], (r, (zp, zm, zd)[i], y, t)
        )

    def y_copy(k, j):
        at = place(k, line[j], y)
        a = share(k, edge) if j == 0 else at
        return push(a, at, y_send.at[k - 2, j], w_recv.at[k, line[j] * 2 + y], beside)

    def landed(k, j, ys):
        at = place(k, line[j], ys)
        push(at, at, y_send.at[k - 2, j], w_recv.at[k, line[j] * 2 + ys], beside).wait_recv()

    def through(k, j):
        return edge == 0 and k == 2 and j == 1

    def arrive(k, j):
        landed(k, j, y)
        if not through(k, j):
            y_copy(k, j).start()

    def lend():
        return push(share(2, 0), swap, swap_sem.at[0], swap_sem.at[1], beside)

    def lent():
        return push(swap, place(2, z, 1 - y, 0), swap_sem.at[2], w_recv.at[2, z * 2 + 1 - y], partner[1])

    def at(point):
        for what, k, i in PLAN[edge].get(point, ()):
            if what == SEND:
                w_copy(k, i).start()
            elif what == OWN:
                y_copy(k, 0).start()
            elif what == TAKE:
                arrive(k, i)
            elif what == LEND:
                lend().start()
            else:
                lend().wait_recv()
                lent().start()

    def norm(values, gain_ref):
        inverse = lax.rsqrt(jnp.mean(values * values, axis=-1, keepdims=True) + eps)
        return (values * inverse * gain_ref[...]).astype(bf16)

    def slot(buf, s, core):
        return buf.at[pl.ds(al((s * 2 + core) * rows, rows), rows), :]

    def ag_copy(g, buf, i):
        s, core, where = (
            (own[g], t, partner[g]), (own[g], t, across), (own[g], t, sibling),
            (pal[g], t, across), (pal[g], t, sibling), (cross[g], t, sibling), (diag[g], t, sibling),
        )[i]
        at = slot(buf, s, core)
        return push(at, at, ag_send.at[g, i], ag_recv.at[g, s * 2 + core], where)

    def ag_wait(g, buf, s, core):
        at = slot(buf, s, core)
        push(at, at, ag_send.at[g, 0], ag_recv.at[g, s * 2 + core], sibling).wait_recv()

    def ag_start(g, buf):
        for i in range(3):
            ag_copy(g, buf, i).start()

    def ag_relay(g, buf, s, sends):
        ag_wait(g, buf, s, t)
        for i in sends:
            ag_copy(g, buf, i).start()

    def sib_copy(n, s, buf, land, lo, size):
        at = buf.at[pl.ds(al(s * seq + (1 - t) * rows, rows), rows), pl.ds(lo, size)]
        to = land.at[pl.ds(al(s * rows, rows), rows), pl.ds(lo, size)]
        return push(at, to, sib_send.at[n, s], sib_recv.at[n, s], sibling)

    def x_copy(n, j, send, land, lo, size):
        return push(
            send.at[j, :, pl.ds(lo, size)], land.at[j, :, pl.ds(lo, size)], x_send.at[n, j], x_recv.at[n, j], across
        )

    def p_copy(g, n, send, land, lo, size):
        return push(send.at[:, pl.ds(lo, size)], land.at[:, pl.ds(lo, size)], p_send.at[n], p_recv.at[n], partner[g])

    def both(s, buf, land, lo, size):
        return (
            buf[pl.ds(al(s * seq + t * rows, rows), rows), pl.ds(lo, size)].astype(f32)
            + land[pl.ds(al(s * rows, rows), rows), pl.ds(lo, size)].astype(f32)
        )

    mixer = (part, sib, xs, xr, ps, pr)
    ff = (part_ff, sib_ff, xs_ff, xr_ff, ps_ff, pr_ff)

    def reduce_x(g, n, lo, size):
        buf, land, send, xland, _, _ = (mixer, ff)[g]
        for j, s in ((0, diag[g]), (1, cross[g])):
            send[j, :, pl.ds(lo, size)] = both(s, buf, land, lo, size).astype(bf16)
            x_copy(n, j, send, xland, lo, size).start()

    def reduce_p(g, n, lo, size):
        buf, land, send, xland, psend, pland = (mixer, ff)[g]
        x_copy(n, 0, send, xland, lo, size).wait_recv()
        total = both(pal[g], buf, land, lo, size) + xland[0, :, pl.ds(lo, size)].astype(f32)
        psend[:, pl.ds(lo, size)] = total.astype(bf16)
        p_copy(g, n, psend, pland, lo, size).start()

    def reduce_end(g, n, lo, size):
        buf, land, send, xland, psend, pland = (mixer, ff)[g]
        x_copy(n, 1, send, xland, lo, size).wait_recv()
        p_copy(g, n, psend, pland, lo, size).wait_recv()
        return (
            both(own[g], buf, land, lo, size)
            + xland[1, :, pl.ds(lo, size)].astype(f32)
            + pland[:, pl.ds(lo, size)].astype(f32)
        )

    def seq_at(g, i):
        rr = lax.rem(r + 1 + lax.div(i, 2), 2)
        ee = lax.rem(side[g] + 1 + lax.rem(i, 2), 2)
        return rr * 2 + ee

    barrier = pltpu.get_barrier_semaphore()
    peers = (sibling, beside, across, partner[1], (r, zm, y, t), (r, zd, y, t))
    for where in peers:
        pl.semaphore_signal(barrier, inc=1, device_id=where, device_id_type=pl.DeviceIdType.MESH)
    for copy in other_trio + own_trio + own_rest[1:]:
        copy.start()
    slot(toks, own[0], t)[...] = norm(tok_ref[...].astype(f32), mix_gain_ref)
    pl.semaphore_wait(barrier, len(peers))
    for copy in other_trio:
        copy.wait()
    near_copy(0).start()
    near_copy(1).start()
    for copy in own_trio:
        copy.wait()
    send_on(0, z, y)
    own_rest[1].wait()
    send_on(1, z, y)
    ag_start(0, toks)
    at(0)
    for k in (0, 1):
        mix_landed(k, z, 1 - y)
    at(1)
    for k in (0, 1):
        for ys in (y, 1 - y):
            mix_landed(k, nth(1), ys)
    at(2)
    for k in (0, 1):
        for ys in (y, 1 - y):
            mix_landed(k, nth(2), ys)
    at(3)
    ag_relay(0, toks, pal[0], (3, 4))
    ag_relay(0, toks, cross[0], (5,))
    for k in (0, 1):
        for ys in (y, 1 - y):
            mix_landed(k, nth(3), ys)
    at(4)
    ag_relay(0, toks, diag[0], (6,))
    for s in (own[0], cross[0], pal[0], diag[0]):
        ag_wait(0, toks, s, 1 - t)
    at(5)

    mix_cols = outb.shape[1]
    taps = taps_ref[:, pl.ds(al((r * 2 + y) * width, width), width)]

    @pl.loop(0, 4)
    def _(i):
        s = seq_at(0, i)
        x = toks[pl.ds(al(s * seq, seq), seq), :]
        proj = jnp.dot(x, trio[...], preferred_element_type=f32).astype(bf16).astype(f32)
        gated = proj[:, 2 * width :] * proj[:, :width]
        row = lax.broadcasted_iota(jnp.int32, gated.shape, 0)
        back1 = jnp.where(row < 1, 0.0, pltpu.roll(gated, 1, 0))
        back2 = jnp.where(row < 2, 0.0, pltpu.roll(gated, 2, 0))
        convolved = taps[0:1] * back2 + taps[1:2] * back1 + taps[2:3] * gated
        mixed = (proj[:, width : 2 * width] * convolved).astype(bf16)
        for lo in range(0, mix_cols, 1024):
            size = min(1024, mix_cols - lo)
            part[pl.ds(al(s * seq, seq), seq), pl.ds(lo, size)] = jnp.dot(
                mixed, outb[:, pl.ds(lo, size)], preferred_element_type=f32
            ).astype(bf16)
        sib_copy(0, s, part, sib, 0, mix_cols).start()

    for s in (diag[0], cross[0]):
        sib_copy(0, s, part, sib, 0, mix_cols).wait_recv()
    for n in range(far):
        reduce_x(0, n, n * group, group)
    at(6)
    for s in (pal[0], own[0]):
        sib_copy(0, s, part, sib, 0, mix_cols).wait_recv()
    for n in range(far):
        reduce_p(0, n, n * group, group)
        at(7 + n)
    for n in range(far):
        span = pl.ds(n * group, group)
        total = reduce_end(0, n, n * group, group)
        resid[:, span] = (tok_ref[:, span].astype(f32) + total).astype(bf16)
    at(11)
    slot(toks_ff, own[1], t)[...] = norm(resid[...].astype(f32), ff_gain_ref)
    ag_start(1, toks_ff)
    at(12)
    ag_relay(1, toks_ff, pal[1], (3, 4))
    at(13)
    ag_relay(1, toks_ff, cross[1], (5,))
    at(14)
    own_rest[2].wait()
    for j in range(4):
        landed(2, j, 1 - y)
    at(16)

    def up(i):
        s = seq_at(1, 3 - i)
        ag_wait(1, toks_ff, s, 1 - t)
        x = toks_ff[pl.ds(al(s * seq, seq), seq), :]
        for lo, size in ((0, 4 * unit), (4 * unit, hid - 4 * unit)):
            act = jnp.dot(x, upb[:, pl.ds(lo, size)], preferred_element_type=f32)
            hidden[pl.ds(al(s * seq, seq), seq), pl.ds(lo, size)] = jnp.square(jnp.maximum(act, 0.0)).astype(bf16)

    pl.loop(0, 3)(up)
    ag_relay(1, toks_ff, diag[1], (6,))
    at(17)
    up(3)
    at(18)

    def down(j, h):
        m = line[j] * 2 + h
        lo = al(m * cols, cols)

        @pl.loop(0, 4)
        def _(i):
            s = seq_at(1, i)
            part_ff[pl.ds(al(s * seq, seq), seq), pl.ds(lo, cols)] = jnp.dot(
                hidden[pl.ds(al(s * seq, seq), seq), pl.ds(0, hid)],
                dnb[pl.ds(0, hid), pl.ds(lo, cols)],
                preferred_element_type=f32,
            ).astype(bf16)
            sib_copy(1 + m, s, part_ff, sib_ff, lo, cols).start()

    def spread(j, h):
        m = line[j] * 2 + h
        lo = al(m * cols, cols)
        for s in (diag[1], cross[1]):
            sib_copy(1 + m, s, part_ff, sib_ff, lo, cols).wait_recv()
        reduce_x(1, far + m, lo, cols)

    def finish(j, h):
        m = line[j] * 2 + h
        lo = al(m * cols, cols)
        for s in (pal[1], own[1]):
            sib_copy(1 + m, s, part_ff, sib_ff, lo, cols).wait_recv()
        reduce_p(1, far + m, lo, cols)

    def out_copy(j, h, ys):
        span = pl.ds(al(line[j] * group + ys * cols + h * strip, strip), strip)
        return pltpu.make_async_copy(result.at[:, span], o_ref.at[:, span], out_sem.at[(j * 2 + h) * 2 + ys])

    def end(j, h):
        m = line[j] * 2 + h
        total = reduce_end(1, far + m, al(m * cols, cols), cols)
        for ys in range(2):
            span = pl.ds(al(line[j] * group + ys * cols + h * strip, strip), strip)
            result[:, span] = (resid[:, span].astype(f32) + total[:, ys * strip : (ys + 1) * strip]).astype(bf16)
            out_copy(j, h, ys).start()

    own_rest[3].wait()
    own_rest[4].wait()
    own_rest[5].wait()
    def sent_mixer():
        for k in (0, 1):
            near_copy(k).wait_send()
            for zs in range(far):
                for ys in range(2):
                    @pl.when(jnp.logical_and(zs <= z, z + 1 < far))
                    def _():
                        hop(k, zs, ys, 1, right_send).wait_send()

                    @pl.when(jnp.logical_and(zs >= z, z > 0))
                    def _():
                        hop(k, zs, ys, -1, left_send).wait_send()
        for g, buf in ((0, toks), (1, toks_ff)):
            for i in range(7):
                ag_copy(g, buf, i).wait_send()
        for s in range(4):
            sib_copy(0, s, part, sib, 0, mix_cols).wait_send()
        for n in range(far):
            lo = n * group
            for j in range(2):
                x_copy(n, j, xs, xr, lo, group).wait_send()
            p_copy(0, n, ps, pr, lo, group).wait_send()

    def sent_weights(ks):
        for k in ks:
            for i in range(3):
                w_copy(k, i).wait_send()
            for j in range(4):
                if not through(k, j):
                    y_copy(k, j).wait_send()

    def sent_step(j, h):
        m = line[j] * 2 + h
        lo = al(m * cols, cols)
        for s in range(4):
            sib_copy(1 + m, s, part_ff, sib_ff, lo, cols).wait_send()
        for i in range(2):
            x_copy(far + m, i, xs_ff, xr_ff, lo, cols).wait_send()
        p_copy(1, far + m, ps_ff, pr_ff, lo, cols).wait_send()

    steps = STEPS[edge]
    late = LATE
    for n, (j, h) in enumerate(steps):
        if n >= late:
            spread(*steps[n - 1])
        if n == 6:
            sent_mixer()
        if n == 7:
            sent_weights((2,))
            for step in steps[:4]:
                sent_step(*step)
        for k in ((3,), (4, 5))[h]:
            landed(k, j, 1 - y)
        down(j, h)
        at(19 + n)
        if 0 < n < late:
            spread(*steps[n - 1])
        if n > 1:
            finish(*steps[n - 2])
    spread(*steps[-1])
    finish(*steps[-2])
    finish(*steps[-1])
    for step in steps:
        end(*step)

    for j, h in steps:
        for ys in range(2):
            out_copy(j, h, ys).wait()
    sent_weights((3, 4, 5))
    if edge == 1:
        lend().wait_send()
        lent().wait_send()
    for step in steps[4:]:
        sent_step(*step)


def layer_kernel(far, *refs):
    z = lax.axis_index("far")
    inside = lax.rem(lax.div(z, 2) + lax.rem(z, 2), 2) == 1
    pl.when(inside)(functools.partial(chip_kernel, far, 0, *refs))
    pl.when(jnp.logical_not(inside))(functools.partial(chip_kernel, far, 1, *refs))


def fused_layer(far, tokens, mix_gain, conv_in, outer, inner, taps, out_w, ff_gain, up_w, down_w):
    bf16 = jnp.bfloat16
    rows, feat = tokens.shape
    depth, cols = up_w.shape[0], down_w.shape[1]
    width, hid = conv_in.shape[1] // 4, up_w.shape[1] * 9 // 32
    whole = 8 * rows
    vmem = pl.BlockSpec(memory_space=pltpu.VMEM)
    hbm = pl.BlockSpec(memory_space=pl.ANY)
    dma = pltpu.SemaphoreType.DMA
    block = [
        pltpu.VMEM((whole, feat), bf16),
        pltpu.VMEM((4 * rows, feat), bf16),
        pltpu.VMEM((2, rows, feat), bf16),
        pltpu.VMEM((2, rows, feat), bf16),
        pltpu.VMEM((rows, feat), bf16),
        pltpu.VMEM((rows, feat), bf16),
    ]
    return pl.pallas_call(
        functools.partial(layer_kernel, far),
        out_shape=jax.ShapeDtypeStruct((rows, feat), bf16),
        in_specs=[vmem, vmem, hbm, hbm, hbm, vmem, hbm, vmem, hbm, hbm],
        out_specs=hbm,
        scratch_shapes=[
            pltpu.VMEM((far * 2 * depth, 3 * width), bf16),
            pltpu.VMEM((width, far * 2 * cols), bf16),
            pltpu.VMEM((far * 2 * depth, hid), bf16),
            pltpu.VMEM((hid, far * 2 * cols), bf16),
            pltpu.VMEM((depth, 3 * width), bf16),
            pltpu.VMEM((whole, feat), bf16),
            pltpu.VMEM((whole, feat), bf16),
            *block,
            *block,
            pltpu.VMEM((whole, hid), bf16),
            pltpu.VMEM((rows, feat), bf16),
            pltpu.VMEM((rows, feat), bf16),
            dma((16,)),
            pltpu.VMEM((depth, hid), bf16),
            dma((3,)),
            dma((8,)),
            dma((3,)),
            dma((2,)),
            dma((2, far * 2)),
            dma((2, far * 2)),
            dma((4, 3)),
            dma((4, 4)),
            dma((6, far * 2)),
            dma((2, 7)),
            dma((2, 8)),
            dma((1 + 2 * far, 4)),
            dma((1 + 2 * far, 4)),
            dma((3 * far, 2)),
            dma((3 * far, 2)),
            dma((3 * far,)),
            dma((3 * far,)),
        ],
        compiler_params=pltpu.CompilerParams(
            collective_id=0, has_side_effects=True, vmem_limit_bytes=60 * 2**20),
    )(tokens, mix_gain[None], conv_in, outer, inner, taps, out_w, ff_gain[None], up_w, down_w)


def solution(mesh):
    rep, fs, tp = (mesh.shape[name] for name in ("rep", "fs", "tp"))
    near = 2 if fs % 2 == 0 else 1
    mesh4 = Mesh(mesh.devices.reshape(rep, fs // near, near, tp), ("rep", "far", "near", "tp"))
    fs_axes = ("far", "near")
    rows = P(("rep", "far", "near", "tp"), None)
    in_specs = (
        rows,
        P(),
        P(fs_axes, "tp"),
        P(fs_axes, "tp"),
        P(fs_axes, "tp"),
        P(None, "tp"),
        P("tp", fs_axes),
        P(),
        P(fs_axes, "tp"),
        P("tp", fs_axes),
    )

    def body(*args):
        if rep == 2 and near == 2 and tp == 2 and fs == 8:
            return fused_layer(fs // near, *args)
        return on_device(rep, near, tp, *args)

    return jax.shard_map(body, mesh=mesh4, in_specs=in_specs, out_specs=rows, check_vma=False)
```
